128 devices in a mesh: sp: 16 (over z, y), tp: 8 (over x, core).
Axes of the slice: x: 4, y: 4, z: 4, core: 2. Of those that a mesh axis runs over, the one named last changes fastest.
Arguments:
- residual_in: bfloat16 [12288, 2048], P('sp', 'tp'), may hold values from -11 to 11
- queries: bfloat16 [12288, 1024], P('sp', 'tp'), may hold values from -6 to 6
- keys: bfloat16 [12288, 256], P('sp'), may hold values from -6 to 6
- values: bfloat16 [12288, 256], P('sp'), may hold values from -6 to 6
- query_gain: float32 [128], replicated, may hold values from 1.5 to 5
- key_norm_gain: float32 [128], replicated, may hold values from 1.5 to 5
- out_weight: bfloat16 [1024, 2048], P('tp'), may hold values from -0.1875 to 0.1875
- mlp_gain: float32 [2048], replicated, may hold values from 0.1 to 1.9
- gate_weight: bfloat16 [2048, 5632], P('sp', 'tp'), may hold values from -0.125 to 0.125
- up_weight: bfloat16 [2048, 5632], P('sp', 'tp'), may hold values from -0.125 to 0.125
- down_weight: bfloat16 [5632, 2048], P('tp', 'sp'), may hold values from -0.15625 to 0.15625
Outputs:
- layer_out: bfloat16 [12288, 2048], P('sp', 'tp')
The draws below stay inside these ranges and needn't reach their ends.
All inputs are finite; a program needn't handle non-finite values.
Results may differ from the reference program's by a relative error of at most 0.012.
The reference program's roundings to bfloat16 on the way count: a program that leaves them out, or rounds other values in their place, can miss the bound.
Values may be sent and summed in bfloat16 or wider, within the bound.
A program may use at most 64 MiB of HBM per device.

```python
import math
import jax
import jax.numpy as jnp
from jax import lax

D = 2048
HEAD_SIZE = 128
QUERY_HEADS = 8
KEY_VALUE_HEADS = 2
FF = 5632
GRID = 64
TOK_DEV = 768
SEQUENCE_TOKENS = 12288
N_TP = 8


def draw_residual_in(key, part):
    column_scale = 0.5 * 4.0 ** (jnp.arange(D, dtype=jnp.float32) / D)
    rotary_period = jnp.clip(jax.random.normal(jax.random.fold_in(key, 3), (SEQUENCE_TOKENS, D)), -4.0, 4.0)
    return (rotary_period * column_scale).astype(jnp.bfloat16)


def draw_queries(key, part):
    rotary_period = jnp.clip(jax.random.normal(jax.random.fold_in(key, 1), (SEQUENCE_TOKENS, QUERY_HEADS * HEAD_SIZE)), -4.0, 4.0)
    return jnp.clip(rotary_period, -6.0, 6.0).astype(jnp.bfloat16)


def draw_keys(key, part):
    rotary_period = jnp.clip(jax.random.normal(jax.random.fold_in(key, 2), (SEQUENCE_TOKENS, KEY_VALUE_HEADS * HEAD_SIZE)), -4.0, 4.0)
    return jnp.clip(rotary_period, -6.0, 6.0).astype(jnp.bfloat16)


def draw_gain(key, salt):
    return jnp.exp(jax.random.uniform(jax.random.fold_in(key, salt), (HEAD_SIZE,), jnp.float32, math.log(1.5), math.log(3.0)))


def draw_query_gain(key, part):
    return draw_gain(key, 4)


def draw_key_norm_gain(key, part):
    return draw_gain(key, 5)


def steps_of(stream_key, extent, cuts, low, top_value):
    loudness, own = 1.0, jax.random.fold_in(stream_key, 6)
    for dim, shards_of in cuts:
        steps = jnp.exp(jax.random.uniform(jax.random.fold_in(own, dim), (shards_of,), jnp.float32, low / len(cuts), top_value / len(cuts)))
        loudness = loudness * jnp.repeat(steps, extent[dim] // shards_of).reshape([-1 if axis == dim else 1 for axis in range(len(extent))])
    return loudness


def gaussian(key, extent, spread, limit, cuts=(), kind=jnp.bfloat16):
    drawn = jax.random.normal(key, extent, jnp.float32) * spread
    if len(cuts) > 0:
        drawn = steps_of(key, extent, cuts, -0.22, 0.18) * drawn
    return jnp.clip(drawn, min=-limit, max=limit).astype(kind)


def setup_inputs(seed: int = 0) -> dict:
    key_of = jax.random.split(jax.random.key(seed), 12)
    return {
        "residual_in": draw_residual_in(jax.random.fold_in(key_of[11], 71), 0),
        "queries": draw_queries(jax.random.fold_in(key_of[11], 71), 0),
        "keys": draw_keys(jax.random.fold_in(key_of[11], 71), 0),
        "values": gaussian(key_of[3], (SEQUENCE_TOKENS, KEY_VALUE_HEADS * HEAD_SIZE), 1.0, 6.0, ((0, 16),)),
        "query_gain": draw_query_gain(jax.random.fold_in(key_of[11], 71), 0),
        "key_norm_gain": draw_key_norm_gain(jax.random.fold_in(key_of[11], 71), 0),
        "out_weight": gaussian(key_of[6], (QUERY_HEADS * HEAD_SIZE, D), (QUERY_HEADS * HEAD_SIZE) ** -0.5, 0.1875, ((0, 8),)),
        "mlp_gain": jnp.clip(1.0 + 0.18 * jax.random.normal(key_of[7], (D,), jnp.float32), 0.1, 1.9),
        "gate_weight": gaussian(key_of[8], (D, FF), D ** -0.5, 0.125, ((0, 16), (1, 8))),
        "up_weight": gaussian(key_of[9], (D, FF), D ** -0.5, 0.125, ((0, 16), (1, 8))),
        "down_weight": gaussian(key_of[10], (FF, D), (FF // 4) ** -0.5, 0.15625, ((0, 8), (1, 16))),
    }


eps = 1e-06
rotary_base = 10000.0

def apply_rotary(vectors, grid_positions):
    half_size = vectors.shape[-1] // 2
    frequency = rotary_base ** (-jnp.arange(0, half_size, 2, dtype=jnp.float32) / half_size)
    grid_row = (grid_positions // GRID).astype(jnp.float32)
    grid_col = (grid_positions % GRID).astype(jnp.float32)
    angles = jnp.concatenate([grid_row[:, None] * frequency, grid_col[:, None] * frequency], axis=-1)[:, None, :]
    cosine_table = jnp.cos(angles)
    sine_table = jnp.sin(angles)
    first_half = vectors[..., :half_size]
    second_half = vectors[..., half_size:]
    return jnp.concatenate([first_half * cosine_table - second_half * sine_table, first_half * sine_table + second_half * cosine_table], axis=-1)

def per_head_norm(vectors, gain):
    return vectors * lax.rsqrt(lax.optimization_barrier(jnp.mean(vectors * vectors, axis=-1, keepdims=True)) + eps) * gain

def grouped_sum(left, right, groups):
    group_width = left.shape[1] // groups

    def add_group(running, group_index):
        left_part = lax.dynamic_slice_in_dim(left, group_index * group_width, group_width, 1)
        right_part = lax.dynamic_slice_in_dim(right, group_index * group_width, group_width, 0)
        partial_sum = jnp.dot(left_part, right_part, preferred_element_type=jnp.float32)
        rounded = lax.optimization_barrier(partial_sum.astype(jnp.bfloat16))
        return (running + rounded.astype(jnp.float32), None)
    start_value = jnp.zeros((left.shape[0], right.shape[1]), jnp.float32)
    result, ignored = lax.scan(add_group, start_value, jnp.arange(groups, dtype=jnp.int32))
    return result

def reference(residual_in, queries, keys, values, query_gain, key_norm_gain, out_weight, mlp_gain, gate_weight, up_weight, down_weight):
    grid_positions = jnp.arange(SEQUENCE_TOKENS, dtype=jnp.int32)
    queries_per_group = QUERY_HEADS // KEY_VALUE_HEADS
    query_rows = apply_rotary(per_head_norm(queries.astype(jnp.float32).reshape(SEQUENCE_TOKENS, QUERY_HEADS, HEAD_SIZE), query_gain), grid_positions).astype(jnp.bfloat16)
    key_matrix = apply_rotary(per_head_norm(keys.astype(jnp.float32).reshape(SEQUENCE_TOKENS, KEY_VALUE_HEADS, HEAD_SIZE), key_norm_gain), grid_positions).astype(jnp.bfloat16)
    value_matrix = values.reshape(SEQUENCE_TOKENS, KEY_VALUE_HEADS, HEAD_SIZE)
    score_scale = HEAD_SIZE ** (-0.5)

    def one_head(head_index):
        head_queries = lax.dynamic_index_in_dim(query_rows, head_index, 1, keepdims=False)
        shared = head_index // queries_per_group
        head_keys = lax.dynamic_index_in_dim(key_matrix, shared, 1, keepdims=False)
        head_values = lax.dynamic_index_in_dim(value_matrix, shared, 1, keepdims=False)

        def one_block(first_row):
            block_queries = lax.dynamic_slice_in_dim(head_queries, first_row, TOK_DEV, 0)
            scores = jnp.dot(block_queries, head_keys.T, preferred_element_type=jnp.float32) * score_scale
            row_max = lax.optimization_barrier(jnp.max(scores, axis=1, keepdims=True))
            weights = jnp.exp(scores - row_max)
            row_sum = lax.optimization_barrier(jnp.sum(weights, axis=1, keepdims=True))
            weighted = jnp.dot(weights.astype(jnp.bfloat16), head_values, preferred_element_type=jnp.float32)
            return (weighted / row_sum).astype(jnp.bfloat16)
        starts = jnp.arange(0, SEQUENCE_TOKENS, TOK_DEV, dtype=jnp.int32)
        return lax.map(one_block, starts).reshape(SEQUENCE_TOKENS, HEAD_SIZE)
    heads_out = lax.map(one_head, jnp.arange(QUERY_HEADS, dtype=jnp.int32))
    attended = jnp.transpose(heads_out, (1, 0, 2)).reshape(SEQUENCE_TOKENS, QUERY_HEADS * HEAD_SIZE)
    projected = grouped_sum(attended, out_weight, N_TP)
    residual_mid = residual_in.astype(jnp.float32) + projected
    normed = (residual_mid * lax.rsqrt(lax.optimization_barrier(jnp.mean(residual_mid * residual_mid, axis=1, keepdims=True)) + eps) * mlp_gain).astype(jnp.bfloat16)
    gate_out = jnp.dot(normed, gate_weight, preferred_element_type=jnp.float32)
    up_out = jnp.dot(normed, up_weight, preferred_element_type=jnp.float32)
    hidden = (jax.nn.silu(gate_out) * up_out).astype(jnp.bfloat16)
    down_sum = grouped_sum(hidden, down_weight, N_TP)
    return (residual_mid + 0.5 * down_sum).astype(jnp.bfloat16)
```

```python
import functools
import math

import jax
import jax.numpy as jnp
import numpy as np
from jax import lax
from jax.experimental import pallas as pl
from jax.experimental.pallas import tpu as pltpu
from jax.sharding import PartitionSpec as P

D = 2048
HEAD = 128
GRID = 64
ROWS = 768
FF_DEV = 704
EPS = 1e-06
CHUNKS = 3
CT = ROWS // CHUNKS
XR = CT + 16
LOG2E = 1.4426950408889634
SCORE = HEAD ** (-0.5) * LOG2E
MESH = pl.DeviceIdType.MESH
F32 = jnp.float32
BF16 = jnp.bfloat16

ORDER = [(0, 0), (0, 3), (3, 0), (0, 1), (1, 0), (0, 2), (2, 0), (3, 3), (3, 1), (1, 3), (1, 1), (3, 2), (2, 3), (1, 2), (2, 1), (2, 2)]
LOOK = 2
GU_AT = 10


def rotary_tables():
    half = HEAD // 2
    freq = (10000.0 ** (-np.arange(0, half, 2, dtype=np.float32) / np.float32(half))).astype(np.float32)
    lanes = np.arange(HEAD)
    of_row = (lanes % 64) < 32
    sign = np.where(lanes < 64, -1.0, 1.0)
    f = freq[lanes % 32]
    out = []
    for count, mask in ((12288 // GRID, of_row), (GRID, ~of_row)):
        ang = (np.arange(count, dtype=np.float32)[:, None] * f[None, :]).astype(np.float32).astype(np.float64)
        out.append(np.where(mask, np.cos(ang), 0.0).astype(np.float32))
        out.append(np.where(mask, np.sin(ang) * sign, 0.0).astype(np.float32))
    return out


def kernel(
    res_ref, q_ref, k_ref, v_ref, qg_ref, kg_ref, wo_ref, mg_ref, g_ref, u_ref, dw_ref,
    rc_ref, rs_ref, cc_ref, cs_ref,
    out_ref,
    kv, gu, dn, att, wo, xn, hid, tb, ob, rb, sb, pb, fb, rm, qT, m_s, acc,
    kv_ss, kv_rs, w_ss, w_rs, rel_ss, rel_rs, wo_ss, wo_rs, at_ss, at_rs, ad_ss, ad_rs,
    xs_ss, xs_rs, xd_ss, xd_rs, td_ss, td_rs, p_ss, p_rs, f_ss, f_rs,
):
    sp = lax.axis_index("sp")
    tp = lax.axis_index("tp")
    z, y = sp // 4, sp % 4
    x, core = tp // 2, tp % 2

    def bid(a, b):
        return ((z + a) % 4) * 4 + (y + b) % 4

    def near(dz, dy):
        return {"sp": bid(dz, dy), "tp": tp}

    def xdev(dx):
        return {"sp": sp, "tp": ((x + dx) % 4) * 2 + core}

    partner_tp = x * 2 + 1 - core
    partner = {"sp": sp, "tp": partner_tp}

    def copy(src, dst, ss, rs, dev):
        return pltpu.make_async_remote_copy(src_ref=src, dst_ref=dst, send_sem=ss, recv_sem=rs, device_id=dev, device_id_type=MESH)

    def when(cond, fn):
        if isinstance(cond, (bool, np.bool_)):
            if cond:
                fn()
        else:
            pl.when(cond)(fn)

    barrier = pltpu.get_barrier_semaphore()
    peers = [near(0, 1), near(0, 3), near(1, 0), near(3, 0)]
    peers += [{"sp": sp, "tp": (tp + d) % 8} for d in range(1, 8)]
    for dev in peers:
        pl.semaphore_signal(barrier, inc=1, device_id=dev, device_id_type=MESH)

    def rotated(ref, lane0, gain, g):
        t = ref[g * 64 : (g + 1) * 64, pl.ds(lane0, HEAD)].astype(F32)
        t = t * lax.rsqrt(jnp.mean(t * t, axis=1, keepdims=True) + EPS) * gain
        grid_row = sp * (ROWS // GRID) + g
        cos = rc_ref[pl.ds(grid_row, 1), :] + cc_ref[...]
        sin = rs_ref[pl.ds(grid_row, 1), :] + cs_ref[...]
        return t * cos + pltpu.roll(t, 64, 1) * sin

    lane0 = pl.multiple_of((tp // 4) * HEAD, HEAD)
    kgain = kg_ref[...]
    qgain = qg_ref[...]
    for g in range(ROWS // GRID):
        kv[0, sp, g // 2, pl.ds((g % 2) * 64, 64), :] = rotated(k_ref, lane0, kgain, g).astype(BF16)
    for i in range(6):
        vi = v_ref[i * 128 : (i + 1) * 128, pl.ds(lane0, HEAD)].astype(F32)
        kv[1, sp, i] = vi.T.astype(BF16)

    pl.semaphore_wait(barrier, len(peers))

    def gather(piece, ss, rs, first):
        def send(a, b, dz, dy):
            at = ((a - dz + 4) % 4) * 4 + (b - dy + 4) % 4
            ref = piece(bid(a, b))
            copy(ref, ref, ss, rs.at[at], near(dz, dy)).start()

        def step(a, b, own=False):
            u, w = (b, a) if first == "y" else (a, b)
            if not own:
                ref = piece(bid(a, b))
                copy(ref, ref, ss, rs.at[a * 4 + b], near(0, 1)).wait_recv()

            def go(du, dw):
                dz, dy = (dw, du) if first == "y" else (du, dw)
                return lambda: send(a, b, dz, dy)

            if own:
                for du, dw in ((1, 0), (3, 0), (0, 1), (0, 3)):
                    go(du, dw)()
            else:
                even = u % 2 == 0
                if isinstance(u, int):
                    when(w == 0 and u == 3, go(1, 0))
                    when(w == 0 or (w == 3 and even), go(0, 1))
                    when(w == 0 or (w == 1 and not even), go(0, 3))
                else:
                    when((w == 0) & (u == 3), go(1, 0))
                    when((w == 0) | ((w == 3) & even), go(0, 1))
                    when((w == 0) | ((w == 1) & (u % 2 == 1)), go(0, 3))

        def drain():
            ref = piece(pl.ds(0, 15))
            copy(ref, ref, ss, rs.at[0], near(0, 1)).wait_send()

        return step, drain

    kv_a = gather(lambda i: kv.at[core, i, 0:3], kv_ss.at[0], kv_rs.at[0], "y")
    kv_b = gather(lambda i: kv.at[core, i, 3:6], kv_ss.at[1], kv_rs.at[1], "z")
    gu_a = gather(lambda i: gu.at[i, 0:64], w_ss.at[0], w_rs.at[0], "y")
    gu_b = gather(lambda i: gu.at[i, 64:128], w_ss.at[1], w_rs.at[1], "z")
    dn_a = gather(lambda i: dn.at[i, 0:352], w_ss.at[2], w_rs.at[2], "y")
    dn_b = gather(lambda i: dn.at[i, 352:704], w_ss.at[3], w_rs.at[3], "z")

    def kv_step(a, b):
        kv_a[0](a, b)
        kv_b[0](a, b)
        ref = kv.at[core, bid(a, b)]
        copy(ref, ref, rel_ss, rel_rs.at[a * 4 + b], partner).start()

    def kv_relayed(a, b):
        ref = kv.at[1 - core, bid(a, b)]
        copy(ref, ref, rel_ss, rel_rs.at[a * 4 + b], partner).wait_recv()

    def gu_step(a, b, own=False):
        gu_a[0](a, b, own)
        gu_b[0](a, b, own)

    def dn_step(a, b, own=False):
        dn_a[0](a, b, own)
        dn_b[0](a, b, own)

    kv_a[0](0, 0, True)
    kv_b[0](0, 0, True)

    for d in range(1, 8):
        to = (tp + d) % 8
        copy(
            wo_ref.at[:, pl.ds(pl.multiple_of(to * 256, 256), 256)], wo.at[tp], wo_ss, wo_rs.at[8 - d], {"sp": sp, "tp": to}
        ).start()

    for g in range(ROWS // GRID):
        qT[:, g * 64 : (g + 1) * 64] = rotated(q_ref, 0, qgain, g).T.astype(BF16)
    m_s[...] = jnp.full_like(m_s, -1e30)
    acc[...] = jnp.zeros_like(acc)

    for n in range(5):
        gu[sp, :, n * 256 : n * 256 + 128] = g_ref[:, n * 128 : (n + 1) * 128]
        gu[sp, :, n * 256 + 128 : (n + 1) * 256] = u_ref[:, n * 128 : (n + 1) * 128]
    gu[sp, :, 1280:1408] = jnp.concatenate([g_ref[:, 640:704], u_ref[:, 640:704]], axis=1)
    dn[sp, 0:704, :] = dw_ref[...]
    for i in range(16):
        dn[i, 704:768, :] = jnp.zeros((64, 128), BF16)
    wo[tp] = wo_ref[:, pl.ds(pl.multiple_of(tp * 256, 256), 256)]

    def attend(blk):
        k = kv[0, blk].reshape(ROWS, HEAD)
        s = jnp.dot(k, qT[...], preferred_element_type=F32)
        old = m_s[...]
        new = jnp.maximum(old, jnp.max(s, axis=0, keepdims=True))
        factor = jnp.exp2((old - new) * SCORE)
        m_s[...] = new
        p = jnp.exp2((s - new) * SCORE).astype(BF16)
        v = kv[1, blk]
        vt = jnp.concatenate([v[i] for i in range(6)], axis=1)
        vt = jnp.concatenate([vt, jnp.ones((16, ROWS), BF16)], axis=0)
        acc[...] = acc[...] * factor + jnp.dot(vt, p, preferred_element_type=F32)

    def place(s):
        a, b = jnp.int32(0), jnp.int32(0)
        for i, (ai, bi) in enumerate(ORDER):
            a = jnp.where(s == i, ai, a)
            b = jnp.where(s == i, bi, b)
        return a, b

    attend(sp)
    for i in range(1, 1 + LOOK):
        kv_step(*ORDER[i])

    def att_loop(s, c):
        @pl.when(s + LOOK < 16)
        def _():
            kv_step(*place(s + LOOK))

        @pl.when(s == GU_AT)
        def _():
            gu_step(0, 0, True)

        @pl.when(s > GU_AT)
        def _():
            gu_step(*place(s - GU_AT))

        a, b = place(s)
        kv_relayed(a, b)
        attend(bid(a, b))
        return c

    lax.fori_loop(1, 16, att_loop, 0)

    todo = [functools.partial(gu_step, *ORDER[i]) for i in range(16 - GU_AT, 11)]
    todo += [functools.partial(dn_step, 0, 0, True)]
    todo += [functools.partial(gu_step, *ORDER[i]) for i in range(11, 16)]
    gu_left = len(todo)
    todo += [functools.partial(dn_step, *ORDER[i]) for i in range(1, 16)]
    done = [0]

    def pump(upto):
        while done[0] < upto:
            todo[done[0]]()
            done[0] += 1

    attn = (acc[0:HEAD, :] / acc[HEAD : HEAD + 1, :]).T.astype(BF16)
    att[tp] = attn

    def xgather(block, pieces, ss, rs, dss, drs):
        def own(dx):
            return ((x + dx) % 4) * 2 + core

        def send(dx, p, to):
            ref = block(own(dx), pieces[p])
            copy(ref, ref, ss.at[p], rs.at[((dx - to) % 4) * 2 + p], xdev(to)).start()

        def wait(dx, p):
            ref = block(own(dx), pieces[p])
            copy(ref, ref, ss.at[p], rs.at[(dx % 4) * 2 + p], xdev(1)).wait_recv()

        whole = (0, pieces[1][1])

        def relay(dx):
            ref = block(own(dx), whole)
            copy(ref, ref, dss, drs.at[dx % 4], partner).start()

        def start():
            send(0, 0, 1)
            send(0, 1, 3)
            send(0, 1, 1)
            send(0, 0, 3)
            relay(0)

        def forward():
            wait(3, 0)
            send(3, 0, 1)
            wait(1, 1)
            send(1, 1, 3)

        def finish():
            wait(3, 1)
            relay(3)
            wait(1, 0)
            relay(1)
            wait(2, 0)
            wait(2, 1)
            relay(2)

        def relayed():
            for dx in (0, 3, 1, 2):
                ref = block(((x + dx) % 4) * 2 + 1 - core, whole)
                copy(ref, ref, dss, drs.at[dx], partner).wait_recv()

        def drain():
            for p in range(2):
                ref = block(pl.ds(0, 3), pieces[p])
                copy(ref, ref, ss.at[p], rs.at[0], xdev(1)).wait_send()
            ref = block(pl.ds(0, 4), whole)
            copy(ref, ref, dss, drs.at[0], partner).wait_send()

        return start, forward, finish, relayed, drain

    def rows_of(ref):
        return lambda i, r: ref.at[i, r[0] : r[1]]

    at_x = xgather(rows_of(att), ((0, 384), (384, 768)), at_ss, at_rs, ad_ss, ad_rs)
    xn_x = [
        xgather(rows_of(xn.at[t]), ((0, 128), (128, XR)), xs_ss.at[t], xs_rs.at[t], xd_ss.at[t], xd_rs.at[t])
        for t in range(CHUNKS)
    ]
    at_x[0]()
    pump(2)
    at_x[1]()
    for d in range(1, 8):
        frm = (tp + d) % 8
        copy(wo.at[frm], wo.at[frm], wo_ss, wo_rs.at[d], {"sp": sp, "tp": frm}).wait_recv()
    pump(4)
    at_x[2]()
    at_x[3]()

    mgain = mg_ref[:, pl.ds(pl.multiple_of(tp * 256, 256), 256)]

    def project(t):
        rows = slice(t * CT, (t + 1) * CT)
        left = jnp.concatenate([att[i, rows] for i in range(8)], axis=1)
        mid = res_ref[rows, :].astype(F32) + jnp.dot(left, wo[...].reshape(8 * HEAD, 256), preferred_element_type=F32)
        rm[rows, :] = mid
        xn[t, tp, 0:CT, :] = (mid * mgain).astype(BF16)
        sq = jnp.sum((mid * mid).T, axis=0, keepdims=True)
        hi = sq.astype(BF16).astype(F32)
        row = lax.broadcasted_iota(jnp.int32, (16, CT), 0)
        xn[t, tp, CT:XR, :] = jnp.where(row == 0, hi, jnp.where(row == 1, sq - hi, 0.0)).astype(BF16)

    for t in range(CHUNKS):
        project(t)
        xn_x[t][0]()

    def gate_up(t):
        total = jnp.zeros((16, CT), F32)
        for i in range(8):
            total = total + xn[t, i, CT:XR, :].astype(F32)
        total = total[0:1, :] + total[1:2, :]
        scale = lax.rsqrt(total / D + EPS)
        scale = jnp.broadcast_to(scale, (128, CT)).T
        left = jnp.concatenate([xn[t, i, 0:CT, :] for i in range(8)], axis=1)

        def tile(n, c):
            w = gu[:, :, pl.ds(pl.multiple_of(n * 256, 256), 256)].reshape(D, 256)
            o = jnp.dot(left, w, preferred_element_type=F32)
            gate, up = o[:, 0:128] * scale, o[:, 128:256] * scale
            hid[t, :, pl.ds(pl.multiple_of(n * 128, 128), 128)] = (gate / (1.0 + jnp.exp(-gate)) * up).astype(BF16)
            return c

        lax.fori_loop(0, 5, tile, 0)
        w = gu[:, :, 1280:1408].reshape(D, 128)
        o = jnp.dot(left, w, preferred_element_type=F32) * scale
        tail = o / (1.0 + jnp.exp(-o)) * pltpu.roll(o, 64, 1)
        lane = lax.broadcasted_iota(jnp.int32, (CT, 128), 1)
        hid[t, :, 640:768] = jnp.where(lane < 64, tail, 0.0).astype(BF16)

    def down(t):
        def term(dst, c_of):
            def tile(dx, c):
                j = ((x + dx) % 4) * 2 + c_of
                w = jnp.concatenate([dn[2 * j], dn[2 * j + 1]], axis=1)
                dst[t, dx] = jnp.dot(hid[t], w, preferred_element_type=F32).astype(BF16)
                return c

            lax.fori_loop(0, 4, tile, 0)

        term(tb, 1 - core)
        copy(tb.at[t], rb.at[t], td_ss.at[t], td_rs.at[t], partner).start()
        term(ob, core)

    def both(t, dx):
        return ob[t, dx].astype(F32) + rb[t, dx].astype(F32)

    def reduce_far(t):
        copy(tb.at[t], rb.at[t], td_ss.at[t], td_rs.at[t], partner).wait_recv()
        sb[t, 0] = both(t, 2).astype(BF16)
        copy(sb.at[t, 0, 0:128], pb.at[t, 0], p_ss.at[t, 0], p_rs.at[t, 0], xdev(1)).start()
        copy(sb.at[t, 0, 128:256], pb.at[t, 1], p_ss.at[t, 1], p_rs.at[t, 1], xdev(3)).start()

    def reduce_near(t):
        copy(sb.at[t, 0, 0:128], pb.at[t, 0], p_ss.at[t, 0], p_rs.at[t, 0], xdev(1)).wait_recv()
        s = both(t, 1)
        sb[t, 1, 0:128, :] = (s[0:128] + pb[t, 0].astype(F32)).astype(BF16)
        sb[t, 1, 128:256, :] = s[128:256].astype(BF16)
        copy(sb.at[t, 1], fb.at[t, 0], f_ss.at[t, 0], f_rs.at[t, 0], xdev(1)).start()
        copy(sb.at[t, 0, 128:256], pb.at[t, 1], p_ss.at[t, 1], p_rs.at[t, 1], xdev(3)).wait_recv()
        s = both(t, 3)
        sb[t, 2, 0:128, :] = s[0:128].astype(BF16)
        sb[t, 2, 128:256, :] = (s[128:256] + pb[t, 1].astype(F32)).astype(BF16)
        copy(sb.at[t, 2], fb.at[t, 1], f_ss.at[t, 1], f_rs.at[t, 1], xdev(3)).start()

    def final(t):
        for i, dx in ((0, 1), (1, 3)):
            copy(sb.at[t, i + 1], fb.at[t, i], f_ss.at[t, i], f_rs.at[t, i], xdev(dx)).wait_recv()
        rows = slice(t * CT, (t + 1) * CT)
        total = both(t, 0) + fb[t, 0].astype(F32) + fb[t, 1].astype(F32)
        out_ref[rows, :] = (rm[rows, :] + 0.5 * total).astype(BF16)

    pump(gu_left - 3)
    xn_x[0][1]()
    pump(gu_left)
    xn_x[0][2]()
    xn_x[1][1]()
    xn_x[0][3]()
    gate_up(0)
    pump(gu_left + 5)
    xn_x[1][2]()
    xn_x[2][1]()
    xn_x[1][3]()
    gate_up(1)
    pump(gu_left + 10)
    xn_x[2][2]()
    xn_x[2][3]()
    gate_up(2)
    pump(len(todo))
    down(0)
    reduce_far(0)
    down(1)
    reduce_near(0)
    reduce_far(1)
    down(2)
    reduce_near(1)
    reduce_far(2)
    final(0)
    reduce_near(2)
    final(1)
    final(2)

    for _, drain in (kv_a, kv_b, gu_a, gu_b, dn_a, dn_b):
        drain()
    ref = kv.at[0, 0:15]
    copy(ref, ref, rel_ss, rel_rs.at[0], partner).wait_send()
    copy(wo.at[0:7], wo.at[0:7], wo_ss, wo_rs.at[0], partner).wait_send()
    at_x[4]()
    for t in range(CHUNKS):
        xn_x[t][4]()
        copy(tb.at[t], rb.at[t], td_ss.at[t], td_rs.at[t], partner).wait_send()
        copy(sb.at[t, 0, 0:128], pb.at[t, 0], p_ss.at[t, 0], p_rs.at[t, 0], xdev(1)).wait_send()
        copy(sb.at[t, 0, 128:256], pb.at[t, 1], p_ss.at[t, 1], p_rs.at[t, 1], xdev(3)).wait_send()
        copy(sb.at[t, 1], fb.at[t, 0], f_ss.at[t, 0], f_rs.at[t, 0], xdev(1)).wait_send()
        copy(sb.at[t, 2], fb.at[t, 1], f_ss.at[t, 1], f_rs.at[t, 1], xdev(3)).wait_send()


def on_device(residual_in, queries, keys, values, query_gain, key_norm_gain, out_weight, mlp_gain, gate_weight, up_weight, down_weight):
    tables = [jnp.asarray(t) for t in rotary_tables()]
    dma = pltpu.SemaphoreType.DMA
    vm = pltpu.VMEM
    scratch = [
        vm((2, 16, 6, 128, 128), BF16),
        vm((16, 128, 2 * FF_DEV), BF16),
        vm((16, 768, 128), BF16),
        vm((8, ROWS, HEAD), BF16),
        vm((8, HEAD, 256), BF16),
        vm((CHUNKS, 8, XR, 256), BF16),
        vm((CHUNKS, CT, 768), BF16),
        vm((CHUNKS, 4, CT, 256), BF16),
        vm((CHUNKS, 4, CT, 256), BF16),
        vm((CHUNKS, 4, CT, 256), BF16),
        vm((CHUNKS, 3, CT, 256), BF16),
        vm((CHUNKS, 2, 128, 256), BF16),
        vm((CHUNKS, 2, CT, 256), BF16),
        vm((ROWS, 256), F32),
        vm((HEAD, ROWS), BF16),
        vm((1, ROWS), F32),
        vm((HEAD + 16, ROWS), F32),
        dma((2,)), dma((2, 16)), dma((4,)), dma((4, 16)), dma, dma((16,)), dma, dma((8,)),
        dma((2,)), dma((8,)), dma, dma((4,)),
        dma((CHUNKS, 2)), dma((CHUNKS, 8)), dma((CHUNKS,)), dma((CHUNKS, 4)),
        dma((CHUNKS,)), dma((CHUNKS,)), dma((CHUNKS, 2)), dma((CHUNKS, 2)), dma((CHUNKS, 2)), dma((CHUNKS, 2)),
    ]
    return pl.pallas_call(
        kernel,
        out_shape=jax.ShapeDtypeStruct((ROWS, 256), BF16),
        in_specs=[pl.BlockSpec(memory_space=pltpu.VMEM)] * 15,
        out_specs=pl.BlockSpec(memory_space=pltpu.VMEM),
        scratch_shapes=scratch,
        compiler_params=pltpu.CompilerParams(collective_id=0, has_side_effects=True, vmem_limit_bytes=60 * 1024 * 1024),
        name="layer",
    )(
        residual_in, queries, keys, values, query_gain.reshape(1, HEAD), key_norm_gain.reshape(1, HEAD), out_weight,
        mlp_gain.reshape(1, D), gate_weight, up_weight, down_weight, *tables,
    )


def solution(mesh):
    in_specs = (
        P("sp", "tp"), P("sp", "tp"), P("sp", None), P("sp", None), P(), P(), P("tp", None), P(),
        P("sp", "tp"), P("sp", "tp"), P("tp", "sp"),
    )
    return jax.shard_map(on_device, mesh=mesh, in_specs=in_specs, out_specs=P("sp", "tp"), check_vma=False)
```

```python
import functools
import math

import jax
import jax.numpy as jnp
import numpy as np
from jax import lax
from jax.experimental import pallas as pl
from jax.experimental.pallas import tpu as pltpu
from jax.sharding import PartitionSpec as P

D = 2048
HEAD = 128
GRID = 64
ROWS = 768
FF_DEV = 704
EPS = 1e-06
CHUNKS = 3
CT = ROWS // CHUNKS
XR = CT + 16
LOG2E = 1.4426950408889634
SCORE = HEAD ** (-0.5) * LOG2E
MESH = pl.DeviceIdType.MESH
F32 = jnp.float32
BF16 = jnp.bfloat16

ORDER = [(0, 0), (0, 1), (0, 3), (1, 0), (3, 0), (1, 1), (0, 2), (3, 1), (1, 3), (2, 0), (1, 2), (3, 3), (3, 2), (2, 3), (2, 1), (2, 2)]
SCHEDULE = {
    "a1": (("ka", 0, 1), ("ka", 0, 3), ("ka", 1, 0), ("ka", 3, 0), ("kb", 0, 1), ("r", 0, 1), ("kb", 0, 3), ("r", 0, 3), ("kb", 1, 0), ("r", 1, 0), ("kb", 3, 0), ("r", 3, 0),),
    "a2": (("ka", 0, 2), ("ka", 1, 1), ("ka", 3, 1),),
    "a3": (("kb", 1, 1), ("r", 1, 1), ("ka", 1, 3), ("ka", 3, 3), ("kb", 0, 2), ("r", 0, 2),),
    "a5": (("kb", 3, 1), ("r", 3, 1), ("ka", 2, 0), ("kb", 1, 3), ("r", 1, 3), ("kb", 2, 0), ("r", 2, 0), ("o", "ga", 0, 1), ("o", "gb", 1, 0),),
    "a6": (("kb", 1, 2), ("ka", 1, 2), ("r", 1, 2), ("ka", 3, 2), ("kb", 3, 3), ("r", 3, 3), ("o", "ga", 1, 0),),
    "a7": (("o", "ga", 3, 0), ("o", "ga", 0, 3), ("o", "gb", 0, 1),),
    "a8": (("ka", 2, 1), ("kb", 3, 2), ("r", 3, 2), ("kb", 2, 3), ("ga", 3, 0), ("o", "gb", 3, 0), ("o", "gb", 0, 3),),
    "a9": (("ka", 2, 3), ("r", 2, 3), ("gb", 3, 0), ("kb", 2, 1), ("r", 2, 1), ("ga", 0, 3),),
    "a10": (("ga", 1, 0), ("o", "gc", 0, 3),),
    "a11": (("ka", 2, 2), ("gb", 0, 3), ("ga", 0, 1), ("o", "gc", 3, 0),),
    "a12": (("kb", 2, 2), ("r", 2, 2), ("gb", 1, 0), ("ga", 2, 0), ("gb", 0, 1),),
    "a13": (("ga", 1, 3), ("gb", 2, 0), ("gb", 3, 1), ("gb", 3, 3), ("o", "gc", 0, 1),),
    "a14": (("gc", 1, 0), ("o", "gd", 3, 0),),
    "a15": (("ga", 3, 3), ("ga", 0, 2), ("gc", 0, 1),),
    "p0": (("ga", 1, 1), ("ga", 3, 1), ("gb", 1, 1), ("gb", 0, 2), ("o", "gc", 1, 0),),
    "p1": (("ga", 2, 3), ("gb", 2, 1), ("gb", 1, 3), ("gc", 3, 0), ("o", "gd", 0, 1), ("gd", 1, 0), ("ga", 3, 2), ("gb", 3, 2), ("gb", 2, 3), ("ga", 1, 2),),
    "p2": (("gc", 3, 1), ("gc", 0, 2), ("gc", 0, 3), ("o", "gd", 0, 3), ("gc", 1, 1), ("gb", 1, 2), ("gc", 2, 0), ("gd", 0, 3), ("ga", 2, 1),),
    "p3": (("ga", 2, 2), ("gd", 1, 1), ("gd", 1, 3), ("o", "gd", 1, 0),),
    "p4": (("gb", 2, 2), ("gd", 2, 0), ("gc", 3, 2), ("gd", 0, 1), ("gc", 1, 2), ("gc", 3, 3), ("gd", 1, 2), ("gd", 0, 2),),
    "p5": (("gc", 1, 3), ("gd", 3, 0), ("gd", 2, 1), ("gd", 2, 3), ("o", "da", 3, 0), ("o", "da", 0, 1), ("o", "da", 0, 3), ("o", "db", 1, 0), ("gc", 2, 1), ("o", "db", 3, 0), ("gc", 2, 2), ("o", "da", 1, 0), ("o", "db", 0, 3), ("gc", 2, 3), ("gd", 3, 1), ("gd", 3, 3), ("o", "db", 0, 1), ("da", 3, 0), ("da", 1, 0), ("gd", 2, 2), ("da", 0, 1), ("db", 3, 0), ("db", 1, 0), ("da", 0, 3), ("db", 0, 1),),
    "p7": (("da", 2, 0), ("gd", 3, 2), ("db", 0, 3), ("da", 1, 1),),
    "p9": (("da", 3, 1), ("da", 0, 2), ("db", 3, 3), ("da", 1, 3), ("db", 2, 0),),
    "p11": (("db", 1, 3), ("db", 3, 1), ("da", 2, 1), ("da", 3, 3),),
    "p13": (("db", 0, 2), ("db", 1, 1), ("da", 1, 2), ("da", 3, 2), ("db", 2, 1), ("db", 2, 3),),
    "p14": (("da", 2, 3), ("db", 3, 2),),
    "p15": (("db", 1, 2), ("da", 2, 2), ("db", 2, 2),),
}
MIRRORED = ("kb", "gc", "gd", "da")


def rotary_tables():
    half = HEAD // 2
    freq = (10000.0 ** (-np.arange(0, half, 2, dtype=np.float32) / np.float32(half))).astype(np.float32)
    lanes = np.arange(HEAD)
    of_row = (lanes % 64) < 32
    sign = np.where(lanes < 64, -1.0, 1.0)
    f = freq[lanes % 32]
    out = []
    for count, mask in ((12288 // GRID, of_row), (GRID, ~of_row)):
        ang = (np.arange(count, dtype=np.float32)[:, None] * f[None, :]).astype(np.float32).astype(np.float64)
        out.append(np.where(mask, np.cos(ang), 0.0).astype(np.float32))
        out.append(np.where(mask, np.sin(ang) * sign, 0.0).astype(np.float32))
    return out


def kernel(
    res_ref, q_ref, k_ref, v_ref, qg_ref, kg_ref, wo_ref, mg_ref, g_ref, u_ref, dw_ref,
    rc_ref, rs_ref, cc_ref, cs_ref,
    out_ref,
    kv, gu, dn, att, wo, xn, hid, tb, ob, rb, sb, pb, fb, rm, qT, m_s, acc,
    kv_ss, kv_rs, w_ss, w_rs, rel_ss, rel_rs, wo_ss, wo_rs, at_ss, at_rs, ad_ss, ad_rs,
    xs_ss, xs_rs, xd_ss, xd_rs, td_ss, td_rs, p_ss, p_rs, f_ss, f_rs,
):
    sp = lax.axis_index("sp")
    tp = lax.axis_index("tp")
    z, y = sp // 4, sp % 4
    x, core = tp // 2, tp % 2

    def bid(a, b):
        return ((z + a) % 4) * 4 + (y + b) % 4

    def near(dz, dy):
        return {"sp": bid(dz, dy), "tp": tp}

    def xdev(dx):
        return {"sp": sp, "tp": ((x + dx) % 4) * 2 + core}

    partner_tp = x * 2 + 1 - core
    partner = {"sp": sp, "tp": partner_tp}

    def copy(src, dst, ss, rs, dev):
        return pltpu.make_async_remote_copy(src_ref=src, dst_ref=dst, send_sem=ss, recv_sem=rs, device_id=dev, device_id_type=MESH)

    barrier = pltpu.get_barrier_semaphore()
    peers = [near(0, 1), near(0, 3), near(1, 0), near(3, 0)]
    peers += [{"sp": sp, "tp": (tp + d) % 8} for d in range(1, 8)]
    for dev in peers:
        pl.semaphore_signal(barrier, inc=1, device_id=dev, device_id_type=MESH)

    def rotated(ref, lane0, gain, g):
        t = ref[g * 64 : (g + 1) * 64, pl.ds(lane0, HEAD)].astype(F32)
        t = t * lax.rsqrt(jnp.mean(t * t, axis=1, keepdims=True) + EPS) * gain
        grid_row = sp * (ROWS // GRID) + g
        cos = rc_ref[pl.ds(grid_row, 1), :] + cc_ref[...]
        sin = rs_ref[pl.ds(grid_row, 1), :] + cs_ref[...]
        return t * cos + pltpu.roll(t, 64, 1) * sin

    lane0 = pl.multiple_of((tp // 4) * HEAD, HEAD)
    kgain = kg_ref[...]
    qgain = qg_ref[...]
    for g in range(ROWS // GRID):
        kv[0, sp, g // 2, pl.ds((g % 2) * 64, 64), :] = rotated(k_ref, lane0, kgain, g).astype(BF16)
    for i in range(6):
        vi = v_ref[i * 128 : (i + 1) * 128, pl.ds(lane0, HEAD)].astype(F32)
        kv[1, sp, i] = vi.T.astype(BF16)

    with jax.named_scope("barrier"):
        pl.semaphore_wait(barrier, len(peers))

    pieces = {
        "ka": (lambda i: kv.at[core, i, 0:3], kv_ss.at[0], kv_rs.at[0]),
        "kb": (lambda i: kv.at[core, i, 3:6], kv_ss.at[1], kv_rs.at[1]),
        "da": (lambda i: dn.at[i, 0:352], w_ss.at[4], w_rs.at[4]),
        "db": (lambda i: dn.at[i, 352:704], w_ss.at[5], w_rs.at[5]),
    }
    for n, name in enumerate(("ga", "gb", "gc", "gd")):
        pieces[name] = (lambda i, n=n: gu.at[i, n * 32 : (n + 1) * 32], w_ss.at[n], w_rs.at[n])

    def send(name, a, b, du, dw):
        piece, ss, rs = pieces[name]
        dz, dy = (dw, du) if name[1] in "ac" else (du, dw)
        ref = piece(bid(a, b))
        copy(ref, ref, ss, rs.at[((a - dz) % 4) * 4 + (b - dy) % 4], near(dz, dy)).start()

    def take(name, a, b):
        piece, ss, rs = pieces[name]
        ref = piece(bid(a, b))
        copy(ref, ref, ss, rs.at[a * 4 + b], near(0, 1)).wait_recv()
        u, w = (b, a) if name[1] in "ac" else (a, b)
        if w == 0 and u == 3 and name not in MIRRORED:
            send(name, a, b, 1, 0)
        if w == 0 and u == 1 and name in MIRRORED:
            send(name, a, b, 3, 0)
        if w == 0 or (w == 3 and u % 2 == 0):
            send(name, a, b, 0, 1)
        if w == 0 or (w == 1 and u % 2 == 1):
            send(name, a, b, 0, 3)

    def drain(name):
        piece, ss, rs = pieces[name]
        ref = piece(pl.ds(0, 15))
        copy(ref, ref, ss, rs.at[0], near(0, 1)).wait_send()

    def run(gap):
        with jax.named_scope(f"run_{gap}"):
            for item in SCHEDULE.get(gap, ()):
                if item[0] == "o":
                    send(item[1], 0, 0, item[2], item[3])
                elif item[0] == "r":
                    ref = kv.at[core, bid(item[1], item[2])]
                    copy(ref, ref, rel_ss, rel_rs.at[item[1] * 4 + item[2]], partner).start()
                else:
                    take(*item)

    def kv_relayed(a, b):
        ref = kv.at[1 - core, bid(a, b)]
        copy(ref, ref, rel_ss, rel_rs.at[a * 4 + b], partner).wait_recv()

    for name in ("ka", "kb"):
        for du, dw in ((1, 0), (3, 0), (0, 1), (0, 3)):
            send(name, 0, 0, du, dw)

    for d in range(1, 8):
        to = (tp + d) % 8
        copy(
            wo_ref.at[:, pl.ds(pl.multiple_of(to * 256, 256), 256)], wo.at[tp], wo_ss, wo_rs.at[8 - d], {"sp": sp, "tp": to}
        ).start()

    for g in range(ROWS // GRID):
        qT[:, g * 64 : (g + 1) * 64] = rotated(q_ref, 0, qgain, g).T.astype(BF16)
    m_s[...] = jnp.full_like(m_s, -1e30)
    acc[...] = jnp.zeros_like(acc)

    for n in range(5):
        cols = slice(n * 128, (n + 1) * 128)
        gu[sp, :, n * 256 : n * 256 + 128] = g_ref[cols, :].T
        gu[sp, :, n * 256 + 128 : (n + 1) * 256] = u_ref[cols, :].T
    gu[sp, :, 1280:1408] = jnp.concatenate([g_ref[640:704, :], u_ref[640:704, :]], axis=0).T
    dn[sp, 0:704, :] = dw_ref[...]
    for i in range(16):
        dn[i, 704:768, :] = jnp.zeros((64, 128), BF16)
    wo[tp] = wo_ref[:, pl.ds(pl.multiple_of(tp * 256, 256), 256)]

    def attend(blk):
        k = kv[0, blk].reshape(ROWS, HEAD)
        s = jnp.dot(k, qT[...], preferred_element_type=F32)
        old = m_s[...]
        new = jnp.maximum(old, jnp.max(s, axis=0, keepdims=True))
        factor = jnp.exp2((old - new) * SCORE)
        m_s[...] = new
        p = jnp.exp2((s - new) * SCORE).astype(BF16)
        v = kv[1, blk]
        vt = jnp.concatenate([v[i] for i in range(6)], axis=1)
        vt = jnp.concatenate([vt, jnp.ones((16, ROWS), BF16)], axis=0)
        acc[...] = acc[...] * factor + jnp.dot(vt, p, preferred_element_type=F32)

    def place(s):
        a, b = jnp.int32(0), jnp.int32(0)
        for i, (ai, bi) in enumerate(ORDER):
            a = jnp.where(s == i, ai, a)
            b = jnp.where(s == i, bi, b)
        return a, b

    run("own")
    with jax.named_scope("att_own"):
        attend(sp)

    def att_loop(s, c):
        for i in range(1, 16):
            pl.when(s == i)(functools.partial(run, f"a{i}"))
        a, b = place(s)
        with jax.named_scope("relay_wait"):
            kv_relayed(a, b)
        with jax.named_scope("attend"):
            attend(bid(a, b))
        return c

    lax.fori_loop(1, 16, att_loop, 0)
    run("p0")
    with jax.named_scope("att_out"):
        attn = (acc[0:HEAD, :] / acc[HEAD : HEAD + 1, :]).T.astype(BF16)
        att[tp] = attn

    def xgather(block, pieces, ss, rs, dss, drs):
        def own(dx):
            return ((x + dx) % 4) * 2 + core

        def send(dx, p, to):
            ref = block(own(dx), pieces[p])
            copy(ref, ref, ss.at[p], rs.at[((dx - to) % 4) * 2 + p], xdev(to)).start()

        def wait(dx, p):
            ref = block(own(dx), pieces[p])
            copy(ref, ref, ss.at[p], rs.at[(dx % 4) * 2 + p], xdev(1)).wait_recv()

        whole = (0, pieces[1][1])

        def relay(dx):
            ref = block(own(dx), whole)
            copy(ref, ref, dss, drs.at[dx % 4], partner).start()

        def start():
            send(0, 0, 1)
            send(0, 1, 3)
            send(0, 1, 1)
            send(0, 0, 3)
            relay(0)

        def forward():
            wait(3, 0)
            send(3, 0, 1)
            wait(1, 1)
            send(1, 1, 3)

        def finish():
            wait(3, 1)
            relay(3)
            wait(1, 0)
            relay(1)
            wait(2, 0)
            wait(2, 1)
            relay(2)

        def relayed():
            for dx in (0, 3, 1, 2):
                ref = block(((x + dx) % 4) * 2 + 1 - core, whole)
                copy(ref, ref, dss, drs.at[dx], partner).wait_recv()

        def drain():
            for p in range(2):
                ref = block(pl.ds(0, 3), pieces[p])
                copy(ref, ref, ss.at[p], rs.at[0], xdev(1)).wait_send()
            ref = block(pl.ds(0, 4), whole)
            copy(ref, ref, dss, drs.at[0], partner).wait_send()

        return start, forward, finish, relayed, drain

    def rows_of(ref):
        return lambda i, r: ref.at[i, r[0] : r[1]]

    at_x = xgather(rows_of(att), ((0, 384), (384, 768)), at_ss, at_rs, ad_ss, ad_rs)
    xn_x = [
        xgather(rows_of(xn.at[t]), ((0, 128), (128, XR)), xs_ss.at[t], xs_rs.at[t], xd_ss.at[t], xd_rs.at[t])
        for t in range(CHUNKS)
    ]
    with jax.named_scope("at_x0"):
        at_x[0]()
    run("p1")
    with jax.named_scope("at_x1"):
        at_x[1]()
    for d in range(1, 8):
        frm = (tp + d) % 8
        copy(wo.at[frm], wo.at[frm], wo_ss, wo_rs.at[d], {"sp": sp, "tp": frm}).wait_recv()
    run("p2")
    with jax.named_scope("at_x2"):
        at_x[2]()
    run("p3")
    with jax.named_scope("at_x3"):
        at_x[3]()

    mgain = mg_ref[:, pl.ds(pl.multiple_of(tp * 256, 256), 256)]

    def project(t):
        rows = slice(t * CT, (t + 1) * CT)
        left = jnp.concatenate([att[i, rows] for i in range(8)], axis=1)
        mid = res_ref[rows, :].astype(F32) + jnp.dot(left, wo[...].reshape(8 * HEAD, 256), preferred_element_type=F32)
        rm[rows, :] = mid
        xn[t, tp, 0:CT, :] = (mid * mgain).astype(BF16)
        sq = jnp.sum((mid * mid).T, axis=0, keepdims=True)
        hi = sq.astype(BF16).astype(F32)
        row = lax.broadcasted_iota(jnp.int32, (16, CT), 0)
        xn[t, tp, CT:XR, :] = jnp.where(row == 0, hi, jnp.where(row == 1, sq - hi, 0.0)).astype(BF16)

    with jax.named_scope("project"):
        for t in range(CHUNKS):
            project(t)
            xn_x[t][0]()

    def gate_up(t):
        total = jnp.zeros((16, CT), F32)
        for i in range(8):
            total = total + xn[t, i, CT:XR, :].astype(F32)
        total = total[0:1, :] + total[1:2, :]
        scale = lax.rsqrt(total / D + EPS)
        scale = jnp.broadcast_to(scale, (128, CT)).T
        left = jnp.concatenate([xn[t, i, 0:CT, :] for i in range(8)], axis=1)

        def tile(n, c):
            w = gu[:, :, pl.ds(pl.multiple_of(n * 256, 256), 256)].reshape(D, 256)
            o = jnp.dot(left, w, preferred_element_type=F32)
            gate, up = o[:, 0:128] * scale, o[:, 128:256] * scale
            hid[t, :, pl.ds(pl.multiple_of(n * 128, 128), 128)] = (gate / (1.0 + jnp.exp(-gate)) * up).astype(BF16)
            return c

        lax.fori_loop(0, 5, tile, 0)
        w = gu[:, :, 1280:1408].reshape(D, 128)
        o = jnp.dot(left, w, preferred_element_type=F32) * scale
        tail = o / (1.0 + jnp.exp(-o)) * pltpu.roll(o, 64, 1)
        lane = lax.broadcasted_iota(jnp.int32, (CT, 128), 1)
        hid[t, :, 640:768] = jnp.where(lane < 64, tail, 0.0).astype(BF16)

    def down(t):
        def term(dst, c_of):
            def tile(dx, c):
                j = ((x + dx) % 4) * 2 + c_of
                w = jnp.concatenate([dn[2 * j], dn[2 * j + 1]], axis=1)
                dst[t, dx] = jnp.dot(hid[t], w, preferred_element_type=F32).astype(BF16)
                return c

            lax.fori_loop(0, 4, tile, 0)

        term(tb, 1 - core)
        copy(tb.at[t], rb.at[t], td_ss.at[t], td_rs.at[t], partner).start()
        term(ob, core)

    def both(t, dx):
        return ob[t, dx].astype(F32) + rb[t, dx].astype(F32)

    def reduce_far(t):
        copy(tb.at[t], rb.at[t], td_ss.at[t], td_rs.at[t], partner).wait_recv()
        sb[t, 0] = both(t, 2).astype(BF16)
        copy(sb.at[t, 0, 0:128], pb.at[t, 0], p_ss.at[t, 0], p_rs.at[t, 0], xdev(1)).start()
        copy(sb.at[t, 0, 128:256], pb.at[t, 1], p_ss.at[t, 1], p_rs.at[t, 1], xdev(3)).start()

    def reduce_near(t):
        copy(sb.at[t, 0, 0:128], pb.at[t, 0], p_ss.at[t, 0], p_rs.at[t, 0], xdev(1)).wait_recv()
        s = both(t, 1)
        sb[t, 1, 0:128, :] = (s[0:128] + pb[t, 0].astype(F32)).astype(BF16)
        sb[t, 1, 128:256, :] = s[128:256].astype(BF16)
        copy(sb.at[t, 1], fb.at[t, 0], f_ss.at[t, 0], f_rs.at[t, 0], xdev(1)).start()
        copy(sb.at[t, 0, 128:256], pb.at[t, 1], p_ss.at[t, 1], p_rs.at[t, 1], xdev(3)).wait_recv()
        s = both(t, 3)
        sb[t, 2, 0:128, :] = s[0:128].astype(BF16)
        sb[t, 2, 128:256, :] = (s[128:256] + pb[t, 1].astype(F32)).astype(BF16)
        copy(sb.at[t, 2], fb.at[t, 1], f_ss.at[t, 1], f_rs.at[t, 1], xdev(3)).start()

    def final(t):
        for i, dx in ((0, 1), (1, 3)):
            copy(sb.at[t, i + 1], fb.at[t, i], f_ss.at[t, i], f_rs.at[t, i], xdev(dx)).wait_recv()
        rows = slice(t * CT, (t + 1) * CT)
        total = both(t, 0) + fb[t, 0].astype(F32) + fb[t, 1].astype(F32)
        out_ref[rows, :] = (rm[rows, :] + 0.5 * total).astype(BF16)

    run("p4")
    with jax.named_scope("xn_x01"):
        xn_x[0][1]()
    run("p5")
    with jax.named_scope("xn_x02"):
        xn_x[0][2]()
    run("p6")
    with jax.named_scope("xn_x11"):
        xn_x[1][1]()
    run("p7")
    with jax.named_scope("xn_x03"):
        xn_x[0][3]()
    run("p8")
    with jax.named_scope("gate_up0"):
        gate_up(0)
    run("p9")
    with jax.named_scope("xn_x12"):
        xn_x[1][2]()
    run("p10")
    with jax.named_scope("xn_x21"):
        xn_x[2][1]()
    run("p11")
    with jax.named_scope("xn_x13"):
        xn_x[1][3]()
    run("p12")
    with jax.named_scope("gate_up1"):
        gate_up(1)
    run("p13")
    with jax.named_scope("xn_x22"):
        xn_x[2][2]()
    run("p14")
    with jax.named_scope("xn_x23"):
        xn_x[2][3]()
    with jax.named_scope("gate_up2"):
        gate_up(2)
    run("p15")
    with jax.named_scope("down0"):
        down(0)
    with jax.named_scope("reduce_far0"):
        reduce_far(0)
    with jax.named_scope("down1"):
        down(1)
    with jax.named_scope("reduce_near0"):
        reduce_near(0)
    with jax.named_scope("reduce_far1"):
        reduce_far(1)
    with jax.named_scope("down2"):
        down(2)
    with jax.named_scope("reduce_near1"):
        reduce_near(1)
    with jax.named_scope("reduce_far2"):
        reduce_far(2)
    with jax.named_scope("final0"):
        final(0)
    with jax.named_scope("reduce_near2"):
        reduce_near(2)
    with jax.named_scope("final1"):
        final(1)
    with jax.named_scope("final2"):
        final(2)

    with jax.named_scope("drain"):
        for name in pieces:
            drain(name)
    ref = kv.at[0, 0:15]
    copy(ref, ref, rel_ss, rel_rs.at[0], partner).wait_send()
    copy(wo.at[0:7], wo.at[0:7], wo_ss, wo_rs.at[0], partner).wait_send()
    with jax.named_scope("at_x4"):
        at_x[4]()
    for t in range(CHUNKS):
        xn_x[t][4]()
        copy(tb.at[t], rb.at[t], td_ss.at[t], td_rs.at[t], partner).wait_send()
        copy(sb.at[t, 0, 0:128], pb.at[t, 0], p_ss.at[t, 0], p_rs.at[t, 0], xdev(1)).wait_send()
        copy(sb.at[t, 0, 128:256], pb.at[t, 1], p_ss.at[t, 1], p_rs.at[t, 1], xdev(3)).wait_send()
        copy(sb.at[t, 1], fb.at[t, 0], f_ss.at[t, 0], f_rs.at[t, 0], xdev(1)).wait_send()
        copy(sb.at[t, 2], fb.at[t, 1], f_ss.at[t, 1], f_rs.at[t, 1], xdev(3)).wait_send()


def on_device(residual_in, queries, keys, values, query_gain, key_norm_gain, out_weight, mlp_gain, gate_weight, up_weight, down_weight):
    tables = [jnp.asarray(t) for t in rotary_tables()]
    dma = pltpu.SemaphoreType.DMA
    vm = pltpu.VMEM
    scratch = [
        vm((2, 16, 6, 128, 128), BF16),
        vm((16, 128, 2 * FF_DEV), BF16),
        vm((16, 768, 128), BF16),
        vm((8, ROWS, HEAD), BF16),
        vm((8, HEAD, 256), BF16),
        vm((CHUNKS, 8, XR, 256), BF16),
        vm((CHUNKS, CT, 768), BF16),
        vm((CHUNKS, 4, CT, 256), BF16),
        vm((CHUNKS, 4, CT, 256), BF16),
        vm((CHUNKS, 4, CT, 256), BF16),
        vm((CHUNKS, 3, CT, 256), BF16),
        vm((CHUNKS, 2, 128, 256), BF16),
        vm((CHUNKS, 2, CT, 256), BF16),
        vm((ROWS, 256), F32),
        vm((HEAD, ROWS), BF16),
        vm((1, ROWS), F32),
        vm((HEAD + 16, ROWS), F32),
        dma((2,)), dma((2, 16)), dma((6,)), dma((6, 16)), dma, dma((16,)), dma, dma((8,)),
        dma((2,)), dma((8,)), dma, dma((4,)),
        dma((CHUNKS, 2)), dma((CHUNKS, 8)), dma((CHUNKS,)), dma((CHUNKS, 4)),
        dma((CHUNKS,)), dma((CHUNKS,)), dma((CHUNKS, 2)), dma((CHUNKS, 2)), dma((CHUNKS, 2)), dma((CHUNKS, 2)),
    ]
    return pl.pallas_call(
        kernel,
        out_shape=jax.ShapeDtypeStruct((ROWS, 256), BF16),
        in_specs=[pl.BlockSpec(memory_space=pltpu.VMEM)] * 15,
        out_specs=pl.BlockSpec(memory_space=pltpu.VMEM),
        scratch_shapes=scratch,
        compiler_params=pltpu.CompilerParams(collective_id=0, has_side_effects=True, vmem_limit_bytes=60 * 1024 * 1024),
        name="layer",
    )(
        residual_in, queries, keys, values, query_gain.reshape(1, HEAD), key_norm_gain.reshape(1, HEAD), out_weight,
        mlp_gain.reshape(1, D), gate_weight.T, up_weight.T, down_weight, *tables,
    )


def solution(mesh):
    in_specs = (
        P("sp", "tp"), P("sp", "tp"), P("sp", None), P("sp", None), P(), P(), P("tp", None), P(),
        P("sp", "tp"), P("sp", "tp"), P("tp", "sp"),
    )
    return jax.shard_map(on_device, mesh=mesh, in_specs=in_specs, out_specs=P("sp", "tp"), check_vma=False)
```

```python
import functools
import math

import jax
import jax.numpy as jnp
import numpy as np
from jax import lax
from jax.experimental import pallas as pl
from jax.experimental.pallas import tpu as pltpu
from jax.sharding import PartitionSpec as P

D = 2048
HEAD = 128
GRID = 64
ROWS = 768
FF_DEV = 704
EPS = 1e-06
TT = ROWS // 8
HALF = ROWS // 2

LOG2E = 1.4426950408889634
SCORE = HEAD ** (-0.5) * LOG2E
MESH = pl.DeviceIdType.MESH
F32 = jnp.float32
BF16 = jnp.bfloat16

ORDER = [(0, 0), (3, 0), (1, 0), (0, 1), (0, 3), (3, 3), (2, 0), (1, 3), (1, 1), (0, 2), (3, 1), (3, 2), (2, 3), (2, 1), (1, 2), (2, 2)]
SCHEDULE = {
    "own": (("o", "gd", 1, 0), ("o", "gd", 0, 3),),
    "a1": (("ka", 0, 3), ("ka", 3, 0), ("ka", 0, 1), ("ka", 1, 0), ("o", "ga", 3, 0), ("kb", 3, 0), ("r", 3, 0), ("kb", 1, 0), ("r", 1, 0), ("kb", 0, 1), ("r", 0, 1), ("kb", 0, 3), ("r", 0, 3),),
    "a3": (("ka", 0, 2), ("ka", 1, 3), ("gd", 0, 1), ("gd", 3, 0),),
    "a4": (("ka", 3, 3), ("ga", 0, 1),),
    "a5": (("ka", 1, 1), ("kb", 3, 3), ("r", 3, 3), ("kb", 3, 1), ("ka", 2, 0), ("kb", 2, 0), ("r", 2, 0), ("kb", 1, 3), ("r", 1, 3),),
    "a6": (("o", "gc", 0, 1),),
    "a7": (("kb", 1, 1), ("r", 1, 1), ("kb", 0, 2), ("r", 0, 2), ("ka", 3, 1), ("r", 3, 1), ("ka", 1, 2), ("o", "gd", 0, 1),),
    "a8": (("gd", 3, 1), ("ka", 3, 2), ("o", "ga", 1, 0),),
    "a9": (("ka", 2, 3), ("gd", 3, 3), ("o", "gd", 3, 0),),
    "a10": (("kb", 3, 2), ("r", 3, 2), ("ga", 3, 1), ("o", "gb", 3, 0), ("o", "gb", 1, 0),),
    "a11": (("ga", 1, 1), ("kb", 2, 3), ("r", 2, 3),),
    "a12": (("kb", 2, 1), ("gd", 0, 3), ("ka", 2, 1), ("r", 2, 1), ("gc", 3, 0), ("o", "gc", 3, 0),),
    "a13": (("o", "ga", 0, 1), ("kb", 1, 2), ("r", 1, 2), ("ka", 2, 2), ("o", "ga", 0, 3), ("o", "gc", 1, 0),),
    "a14": (("gd", 1, 0), ("ga", 0, 3),),
    "a15": (("gb", 3, 0), ("kb", 2, 2), ("r", 2, 2), ("gb", 1, 0), ("gd", 3, 2),),
    "p0": (("gc", 2, 0), ("ga", 2, 1), ("gc", 0, 1), ("gd", 0, 2),),
    "p1": (("gd", 1, 1), ("ga", 3, 0), ("gc", 0, 3), ("ga", 1, 0),),
    "p2": (("ga", 3, 3), ("gb", 3, 1), ("gd", 2, 0), ("gd", 1, 3), ("gb", 2, 0), ("gb", 1, 1), ("ga", 0, 2), ("ga", 1, 3), ("gc", 3, 1), ("gc", 0, 2), ("gb", 3, 3), ("gc", 1, 1),),
    "p4": (("gd", 1, 2), ("ga", 2, 0), ("gb", 1, 3), ("gc", 1, 3), ("o", "gb", 0, 1), ("o", "db", 1, 0), ("gc", 3, 3), ("gb", 3, 2), ("o", "da", 3, 0), ("ga", 1, 2), ("gd", 2, 3), ("ga", 3, 2), ("gd", 2, 1), ("ga", 2, 3), ("gb", 2, 3), ("gc", 3, 2), ("gb", 2, 1), ("o", "gb", 0, 3), ("o", "gc", 0, 3), ("o", "db", 3, 0), ("gb", 0, 3), ("gc", 1, 2),),
    "p5": (("o", "da", 1, 0), ("o", "db", 0, 1),),
    "p6": (("db", 3, 0), ("gb", 1, 2), ("gc", 2, 1), ("gd", 2, 2), ("ga", 2, 2), ("da", 0, 1), ("o", "da", 0, 3), ("gb", 2, 2), ("gc", 2, 3),),
    "p7": (("gc", 2, 2), ("gb", 0, 1), ("o", "da", 0, 1), ("gb", 0, 2), ("gc", 1, 0),),
    "g0": (("o", "db", 0, 3),),
    "g1": (("db", 2, 0), ("db", 1, 0), ("db", 3, 1), ("da", 0, 3),),
    "g3": (("da", 0, 2), ("da", 3, 1), ("da", 1, 1), ("db", 0, 3),),
    "p9": (("db", 0, 1), ("da", 3, 0),),
    "i0": (("db", 3, 3), ("da", 1, 0),),
    "p12": (("db", 2, 1), ("da", 3, 3), ("da", 1, 3), ("db", 2, 3), ("da", 3, 2), ("db", 1, 1), ("da", 1, 2), ("db", 1, 3), ("db", 3, 2), ("da", 2, 0), ("da", 2, 1), ("db", 0, 2), ("da", 2, 3), ("da", 2, 2), ("db", 2, 2), ("db", 1, 2),),
}
FAR_AT = 3
MIRRORED = ("kb", "gc", "gd", "da")


def rotary_tables():
    half = HEAD // 2
    freq = (10000.0 ** (-np.arange(0, half, 2, dtype=np.float32) / np.float32(half))).astype(np.float32)
    lanes = np.arange(HEAD)
    of_row = (lanes % 64) < 32
    sign = np.where(lanes < 64, -1.0, 1.0)
    f = freq[lanes % 32]
    out = []
    for count, mask in ((12288 // GRID, of_row), (GRID, ~of_row)):
        ang = (np.arange(count, dtype=np.float32)[:, None] * f[None, :]).astype(np.float32).astype(np.float64)
        out.append(np.where(mask, np.cos(ang), 0.0).astype(np.float32))
        out.append(np.where(mask, np.sin(ang) * sign, 0.0).astype(np.float32))
    return out


def kernel(
    res_h, q_ref, k_ref, v_ref, qg_ref, kg_ref, wo_h, mg_ref, g_h, u_h, dw_h,
    rc_ref, rs_ref, cc_ref, cs_ref,
    out_ref,
    kv, gu, dn, att, att_t, wo, res_t, mid_s, xn, pj, pr, hid, tb, rb, sb, pb, fb, qT, m_s, acc, scores, gu_s, base_s, res_ref, g_ref, u_ref, in_s,
    kv_ss, kv_rs, w_ss, w_rs, rel_ss, rel_rs, wo_ss, wo_rs, wd_ss, wd_rs, res_ss, res_rs, at_ss, at_rs,
    xs_ss, xs_rs, xd_ss, xd_rs, pj_ss, pj_rs, td_ss, td_rs, p_ss, p_rs, f_ss, f_rs,
):
    sp = lax.axis_index("sp")
    tp = lax.axis_index("tp")
    z, y = sp // 4, sp % 4
    x, core = tp // 2, tp % 2

    def bid(a, b):
        return ((z + a) % 4) * 4 + (y + b) % 4

    def near(dz, dy):
        return {"sp": bid(dz, dy), "tp": tp}

    def xdev(dx):
        return {"sp": sp, "tp": ((x + dx) % 4) * 2 + core}

    partner_tp = x * 2 + 1 - core
    partner = {"sp": sp, "tp": partner_tp}

    def copy(src, dst, ss, rs, dev):
        return pltpu.make_async_remote_copy(src_ref=src, dst_ref=dst, send_sem=ss, recv_sem=rs, device_id=dev, device_id_type=MESH)

    barrier = pltpu.get_barrier_semaphore()
    peers = [near(0, 1), near(0, 3), near(1, 0), near(3, 0)]
    peers += [{"sp": sp, "tp": (tp + d) % 8} for d in range(1, 8)]
    for dev in peers:
        pl.semaphore_signal(barrier, inc=1, device_id=dev, device_id_type=MESH)

    loads = [
        pltpu.make_async_copy(res_h, res_ref, in_s.at[0]),
        pltpu.make_async_copy(wo_h, wo.at[tp], in_s.at[1]),
        pltpu.make_async_copy(g_h, g_ref, in_s.at[2]),
        pltpu.make_async_copy(u_h, u_ref, in_s.at[3]),
        pltpu.make_async_copy(dw_h, dn.at[sp, 0:FF_DEV], in_s.at[4]),
    ]
    for load in loads:
        load.start()

    def rotated(ref, lane0, gain, g):
        t = ref[g * 64 : (g + 1) * 64, pl.ds(lane0, HEAD)].astype(F32)
        t = t * lax.rsqrt(jnp.mean(t * t, axis=1, keepdims=True) + EPS) * gain
        grid_row = sp * (ROWS // GRID) + g
        cos = rc_ref[pl.ds(grid_row, 1), :] + cc_ref[...]
        sin = rs_ref[pl.ds(grid_row, 1), :] + cs_ref[...]
        return t * cos + pltpu.roll(t, 64, 1) * sin

    lane0 = pl.multiple_of((tp // 4) * HEAD, HEAD)
    kgain = kg_ref[...]
    qgain = qg_ref[...]
    def own_keys():
        for g in range(ROWS // GRID):
            kv[0, sp, g // 2, pl.ds((g % 2) * 64, 64), :] = rotated(k_ref, lane0, kgain, g).astype(BF16)

    def own_values():
        for i in range(6):
            vi = v_ref[i * 128 : (i + 1) * 128, pl.ds(lane0, HEAD)].astype(F32)
            kv[1, sp, i] = vi.T.astype(BF16)

    pl.when(core == 0)(own_keys)
    pl.when(core == 1)(own_values)

    with jax.named_scope("barrier"):
        pl.semaphore_wait(barrier, len(peers))

    pieces = {
        "ka": (lambda i: kv.at[core, i, 0:3], kv_ss.at[0], kv_rs.at[0]),
        "kb": (lambda i: kv.at[core, i, 3:6], kv_ss.at[1], kv_rs.at[1]),
        "da": (lambda i: dn.at[i, 0:352], w_ss.at[4], w_rs.at[4]),
        "db": (lambda i: dn.at[i, 352:704], w_ss.at[5], w_rs.at[5]),
    }
    for n, name in enumerate(("ga", "gb", "gc", "gd")):
        pieces[name] = (lambda i, n=n: gu.at[i, n * 32 : (n + 1) * 32], w_ss.at[n], w_rs.at[n])

    def send(name, a, b, du, dw):
        piece, ss, rs = pieces[name]
        dz, dy = (dw, du) if name[1] in "ac" else (du, dw)
        ref = piece(bid(a, b))
        copy(ref, ref, ss, rs.at[((a - dz) % 4) * 4 + (b - dy) % 4], near(dz, dy)).start()

    def take(name, a, b):
        piece, ss, rs = pieces[name]
        ref = piece(bid(a, b))
        copy(ref, ref, ss, rs.at[a * 4 + b], near(0, 1)).wait_recv()
        u, w = (b, a) if name[1] in "ac" else (a, b)
        if w == 0 and u == 3 and name not in MIRRORED:
            send(name, a, b, 1, 0)
        if w == 0 and u == 1 and name in MIRRORED:
            send(name, a, b, 3, 0)
        if w == 0 or (w == 3 and u % 2 == 0):
            send(name, a, b, 0, 1)
        if w == 0 or (w == 1 and u % 2 == 1):
            send(name, a, b, 0, 3)

    def drain(name):
        piece, ss, rs = pieces[name]
        ref = piece(pl.ds(0, 15))
        copy(ref, ref, ss, rs.at[0], near(0, 1)).wait_send()

    def run(gap):
        with jax.named_scope(f"run_{gap}"):
            for item in SCHEDULE.get(gap, ()):
                if item[0] == "o":
                    send(item[1], 0, 0, item[2], item[3])
                elif item[0] == "r":
                    ref = kv.at[core, bid(item[1], item[2])]
                    copy(ref, ref, rel_ss, rel_rs.at[item[1] * 4 + item[2]], partner).start()
                else:
                    take(*item)

    def kv_relayed(a, b):
        ref = kv.at[1 - core, bid(a, b)]
        copy(ref, ref, rel_ss, rel_rs.at[a * 4 + b], partner).wait_recv()

    for name in ("ka", "kb"):
        for du, dw in ((1, 0), (3, 0), (0, 1), (0, 3)):
            send(name, 0, 0, du, dw)

    pl.when(core == 1)(own_keys)
    pl.when(core == 0)(own_values)

    def tokens(i):
        return pl.ds(pl.multiple_of(i * TT, TT), TT)

    def exchange(src, dst, ss, rs):
        for d in (1, 2, 7, 6, 3, 5, 4):
            to = (tp + d) % 8
            copy(src(to), dst(tp), ss, rs.at[8 - d], {"sp": sp, "tp": to}).start()

    def exchanged(dst, ss, rs):
        for d in range(1, 8):
            frm = (tp + d) % 8
            copy(dst(frm), dst(frm), ss, rs.at[d], {"sp": sp, "tp": frm}).wait_recv()

    def exchange_drain(dst, ss, rs):
        ref = dst(pl.ds(0, 7))
        copy(ref, ref, ss, rs.at[0], partner).wait_send()

    for load in loads:
        load.wait()
    exchange(lambda i: res_ref.at[tokens(i)], lambda i: res_t.at[i], res_ss, res_rs)

    for g in range(ROWS // GRID):
        qT[:, g * 64 : (g + 1) * 64] = rotated(q_ref, 0, qgain, g).T.astype(BF16)
    m_s[...] = jnp.full_like(m_s, -1e30)
    acc[...] = jnp.zeros_like(acc)

    for n in range(5):
        cols = slice(n * 128, (n + 1) * 128)
        gu[sp, :, n * 256 : n * 256 + 128] = g_ref[cols, :].T
        gu[sp, :, n * 256 + 128 : (n + 1) * 256] = u_ref[cols, :].T
    gu[sp, :, 1280:1408] = jnp.concatenate([g_ref[640:704, :], u_ref[640:704, :]], axis=0).T
    for i in range(16):
        dn[i, 704:768, :] = jnp.zeros((64, 128), BF16)

    def xgather(block, pieces, ss, rs, dss, drs):
        def own(dx):
            return ((x + dx) % 4) * 2 + core

        def send(dx, p, to):
            ref = block(own(dx), pieces[p])
            copy(ref, ref, ss.at[p], rs.at[((dx - to) % 4) * 2 + p], xdev(to)).start()

        def wait(dx, p):
            ref = block(own(dx), pieces[p])
            copy(ref, ref, ss.at[p], rs.at[(dx % 4) * 2 + p], xdev(1)).wait_recv()

        whole = (0, pieces[1][1])

        def relay(dx):
            ref = block(own(dx), whole)
            copy(ref, ref, dss, drs.at[dx % 4], partner).start()

        def start():
            send(0, 0, 1)
            send(0, 1, 3)
            send(0, 1, 1)
            send(0, 0, 3)
            relay(0)

        def forward():
            wait(3, 0)
            send(3, 0, 1)
            wait(1, 1)
            send(1, 1, 3)

        def finish():
            wait(3, 1)
            relay(3)
            wait(1, 0)
            relay(1)

        def finish_far():
            wait(2, 0)
            wait(2, 1)
            relay(2)

        def relayed(which=(0, 3, 1, 2)):
            for dx in which:
                ref = block(((x + dx) % 4) * 2 + 1 - core, whole)
                copy(ref, ref, dss, drs.at[dx], partner).wait_recv()

        def drain():
            for p in range(2):
                ref = block(pl.ds(0, 3), pieces[p])
                copy(ref, ref, ss.at[p], rs.at[0], xdev(1)).wait_send()
            ref = block(pl.ds(0, 4), whole)
            copy(ref, ref, dss, drs.at[0], partner).wait_send()

        return start, forward, finish, finish_far, relayed, drain

    def rows_of(ref):
        return lambda i, r: ref.at[i, r[0] : r[1]]

    wo_start, wo_forward, wo_finish, wo_far, wo_relayed, wo_drain = xgather(
        rows_of(wo), ((0, 64), (64, HEAD)), wo_ss, wo_rs, wd_ss, wd_rs
    )
    xn_start, xn_forward, xn_finish, xn_far, xn_relayed, xn_drain = xgather(
        rows_of(xn), ((0, TT // 2), (TT // 2, TT)), xs_ss, xs_rs, xd_ss, xd_rs
    )
    wo_start()

    def product(blk):
        return jnp.dot(kv[0, blk].reshape(ROWS, HEAD), qT[...], preferred_element_type=F32)

    def absorb(s, blk):
        old = m_s[...]
        new = jnp.maximum(old, jnp.max(s, axis=0, keepdims=True))
        factor = jnp.exp2((old - new) * SCORE)
        m_s[...] = new
        p = jnp.exp2((s - new) * SCORE).astype(BF16)
        v = kv[1, blk]
        vt = jnp.concatenate([v[i] for i in range(6)], axis=1)
        vt = jnp.concatenate([vt, jnp.ones((16, ROWS), BF16)], axis=0)
        acc[...] = acc[...] * factor + jnp.dot(vt, p, preferred_element_type=F32)

    def place(s):
        a, b = jnp.int32(0), jnp.int32(0)
        for i, (ai, bi) in enumerate(ORDER):
            a = jnp.where(s == i, ai, a)
            b = jnp.where(s == i, bi, b)
        return a, b

    run("own")
    with jax.named_scope("att_own"):
        absorb(product(sp), sp)
    run("a1")
    with jax.named_scope("relay_wait"):
        kv_relayed(*ORDER[1])
    with jax.named_scope("first"):
        scores[0] = product(bid(*ORDER[1]))

    def att_loop(i, c):
        for h in range(2):
            s = 2 * i + 1 + h
            for k in range(2 + h, 16, 2):
                pl.when(s == k - 1)(functools.partial(run, f"a{k}"))
            for k, fn in ((3, wo_forward), (9, wo_finish), (13, wo_far)):
                if k % 2 == 1 - h:
                    pl.when(s == k)(fn)
            now, later = place(s), place(s + 1)
            with jax.named_scope("relay_wait"):
                kv_relayed(*later)
            with jax.named_scope("attend"):
                scores[1 - h] = product(bid(*later))
                absorb(scores[h], bid(*now))
        return c

    lax.fori_loop(0, 7, att_loop, 0)
    absorb(scores[0], bid(*ORDER[15]))
    run("p0")
    with jax.named_scope("att_out"):
        attn = (acc[0:HEAD, :] / acc[HEAD : HEAD + 1, :]).T.astype(BF16)
        att[...] = attn

    exchange(lambda i: att.at[tokens(i)], lambda i: att_t.at[i], at_ss, at_rs)
    att_t[tp] = att[tokens(tp)]
    res_t[tp] = res_ref[tokens(tp), :]
    run("p1")
    with jax.named_scope("wo_wait"):
        wo_relayed()
        exchanged(lambda i: res_t.at[i], res_ss, res_rs)
    run("p2")
    with jax.named_scope("att_wait"):
        exchanged(lambda i: att_t.at[i], at_ss, at_rs)

    def project():
        left = jnp.concatenate([att_t[i] for i in range(8)], axis=1)
        squares = jnp.zeros((TT, 1), F32)
        for n in range(4):
            cols = slice(n * 512, (n + 1) * 512)
            p = jnp.dot(left, wo[:, :, cols].reshape(8 * HEAD, 512), preferred_element_type=F32)
            for i in range(2):
                part = p[:, i * 256 : (i + 1) * 256]
                pj[2 * n + i] = part.astype(BF16)
                mid = res_t[2 * n + i].astype(F32) + part
                mid_s[:, n * 512 + i * 256 : n * 512 + (i + 1) * 256] = mid
                squares = squares + jnp.sum(mid * mid, axis=1, keepdims=True)
        scale = lax.rsqrt(squares / D + EPS)
        xn[tp] = (mid_s[...] * scale * mg_ref[...]).astype(BF16)

    with jax.named_scope("project"):
        project()
    xn_start()

    def gate_up(far_by, name):
        chips = [(x + dx) % 4 for dx in far_by]

        def keep(value, lanes):
            for i, c in enumerate(chips):
                rows = pl.ds(pl.multiple_of(c * 2 * TT, 2 * TT), 2 * TT)
                hid[rows, lanes] = value[i * 2 * TT : (i + 1) * 2 * TT].astype(BF16)

        count = len(chips) * 2 * TT

        def silu(n):
            o = gu_s[n % 2, 0:count, :]
            if n < 5:
                gate, up = o[:, 0:128], o[:, 128:256]
                keep(gate / (1.0 + jnp.exp(-gate)) * up, slice(n * 128, (n + 1) * 128))
            else:
                o = o[:, 0:128]
                tail = o / (1.0 + jnp.exp(-o)) * pltpu.roll(o, 64, 1)
                lane = lax.broadcasted_iota(jnp.int32, tail.shape, 1)
                keep(jnp.where(lane < 64, tail, 0.0), slice(640, 768))

        for n in range(6):
            width = 256 if n < 5 else 128
            w = gu[:, :, n * 256 : n * 256 + width].reshape(D, width)
            for i, c in enumerate(chips):
                left = xn[pl.ds(2 * c, 2)].reshape(2 * TT, D)
                gu_s[n % 2, i * 2 * TT : (i + 1) * 2 * TT, 0:width] = jnp.dot(left, w, preferred_element_type=F32)
            if n > 0:
                silu(n - 1)
            if n < 5:
                run(f"{name}{n}")
                if name == "g" and n == FAR_AT:
                    run("gf")
                    with jax.named_scope("xn_far"):
                        xn_far()
        silu(5)

    def down(dx, rows=slice(0, ROWS)):
        j = ((x + dx) % 4) * 4
        w = jnp.concatenate([dn[j + i] for i in range(4)], axis=1)
        o = jnp.dot(hid[rows, :], w, preferred_element_type=F32)
        for c in range(2):
            tb[dx, c, rows] = o[:, c * 256 : (c + 1) * 256].astype(BF16)

    def to_partner(dx):
        return copy(tb.at[dx, 1 - core], rb.at[dx], td_ss.at[dx], td_rs.at[dx], partner)

    def half_to_partner(h):
        rows = pl.ds(h * HALF, HALF)
        return copy(tb.at[2, 1 - core, rows], rb.at[2, rows], td_ss.at[2 + 2 * h], td_rs.at[2 + 2 * h], partner)

    def far(i):
        to = xdev((1, 3)[i])
        return copy(sb.at[0, pl.ds(i * HALF, HALF)], pb.at[i], p_ss.at[i], p_rs.at[i], to)

    def close(i, h):
        to = xdev((1, 3)[i])
        rows = pl.ds(h * HALF, HALF)
        return copy(sb.at[1 + i, rows], fb.at[i, rows], f_ss.at[i, h], f_rs.at[i, h], to)

    def both(dx, h):
        rows = slice(h * HALF, (h + 1) * HALF)
        return tb[dx, core, rows].astype(F32) + rb[dx, rows].astype(F32)

    def reduce_far(i):
        half_to_partner(i).wait_recv()
        sb[0, i * HALF : (i + 1) * HALF] = both(2, i).astype(BF16)
        far(i).start()

    def reduce_free(i):
        dx, h = (1, 3)[i], 1 - i
        to_partner(dx).wait_recv()
        sb[1 + i, h * HALF : (h + 1) * HALF] = both(dx, h).astype(BF16)
        close(i, h).start()

    def reduce_near(i):
        dx, h = (1, 3)[i], i
        s = both(dx, h)
        far(i).wait_recv()
        sb[1 + i, h * HALF : (h + 1) * HALF] = (s + pb[i].astype(F32)).astype(BF16)
        close(i, h).start()

    def begin(h):
        rows = slice(h * HALF, (h + 1) * HALF)
        i = 1 - h
        close(i, h).wait_recv()
        mid = res_ref[rows, :].astype(F32) + pr[h * 4 : h * 4 + 4].reshape(HALF, 256).astype(F32)
        base_s[rows, :] = mid + 0.5 * (both(0, h) + fb[i, rows].astype(F32))

    def final(h):
        rows = slice(h * HALF, (h + 1) * HALF)
        close(h, h).wait_recv()
        out_ref[rows, :] = (base_s[rows, :] + 0.5 * fb[h, rows].astype(F32)).astype(BF16)

    run("p4")
    with jax.named_scope("xn_forward"):
        xn_forward()
    with jax.named_scope("exchangelambdaipja"):
        exchange(lambda i: pj.at[i], lambda i: pr.at[i], pj_ss, pj_rs)
    with jax.named_scope("prtppjtp"):
        pr[tp] = pj[tp]
    run("p5")
    with jax.named_scope("xn_relayed_own"):
        xn_relayed((0,))
    run("p6")
    with jax.named_scope("xn_finish"):
        xn_finish()
    run("p7")
    with jax.named_scope("xn_relayed"):
        xn_relayed((3, 1))
    run("p8")
    with jax.named_scope("gate_up"):
        gate_up((0, 3, 1), "g")
    run("p9")
    with jax.named_scope("xn_relayed_far"):
        xn_relayed((2,))
    with jax.named_scope("gate_up_far"):
        gate_up((2,), "i")
    run("p12")
    with jax.named_scope("down2"):
        down(2, slice(0, HALF))
        half_to_partner(0).start()
        down(2, slice(HALF, ROWS))
        half_to_partner(1).start()
    with jax.named_scope("down1"):
        down(1)
        to_partner(1).start()
    with jax.named_scope("reduce_far"):
        reduce_far(0)
        reduce_far(1)
    with jax.named_scope("down3"):
        down(3)
        to_partner(3).start()
    with jax.named_scope("reduce_free0"):
        reduce_free(0)
    with jax.named_scope("reduce_free1"):
        reduce_free(1)
    with jax.named_scope("down0"):
        down(0)
        to_partner(0).start()
    with jax.named_scope("reduce_near0"):
        reduce_near(0)
    with jax.named_scope("reduce_near1"):
        reduce_near(1)
    with jax.named_scope("to_partner0wait_re"):
        to_partner(0).wait_recv()
    with jax.named_scope("exchangedlambdaipr"):
        exchanged(lambda i: pr.at[i], pj_ss, pj_rs)
    with jax.named_scope("begin"):
        begin(0)
        begin(1)
    with jax.named_scope("final0"):
        final(0)
    with jax.named_scope("final1"):
        final(1)

    with jax.named_scope("drain"):
        for name in pieces:
            drain(name)
    ref = kv.at[0, 0:15]
    copy(ref, ref, rel_ss, rel_rs.at[0], partner).wait_send()
    exchange_drain(lambda i: res_t.at[i], res_ss, res_rs)
    exchange_drain(lambda i: att_t.at[i], at_ss, at_rs)
    exchange_drain(lambda i: pr.at[i], pj_ss, pj_rs)
    wo_drain()
    xn_drain()
    for dx in (0, 1, 3):
        to_partner(dx).wait_send()
    for i in range(2):
        half_to_partner(i).wait_send()
        far(i).wait_send()
        close(i, 0).wait_send()
        close(i, 1).wait_send()


def on_device(residual_in, queries, keys, values, query_gain, key_norm_gain, out_weight, mlp_gain, gate_weight, up_weight, down_weight):
    tables = [jnp.asarray(t) for t in rotary_tables()]
    dma = pltpu.SemaphoreType.DMA
    vm = pltpu.VMEM
    scratch = [
        vm((2, 16, 6, 128, 128), BF16),
        vm((16, 128, 2 * FF_DEV), BF16),
        vm((16, 768, 128), BF16),
        vm((ROWS, HEAD), BF16),
        vm((8, TT, HEAD), BF16),
        vm((8, HEAD, D), BF16),
        vm((8, TT, 256), BF16),
        vm((TT, D), F32),
        vm((8, TT, D), BF16),
        vm((8, TT, 256), BF16),
        vm((8, TT, 256), BF16),
        vm((ROWS, 768), BF16),
        vm((4, 2, ROWS, 256), BF16),
        vm((4, ROWS, 256), BF16),
        vm((3, ROWS, 256), BF16),
        vm((2, HALF, 256), BF16),
        vm((2, ROWS, 256), BF16),
        vm((HEAD, ROWS), BF16),
        vm((1, ROWS), F32),
        vm((HEAD + 16, ROWS), F32),
        vm((2, ROWS, ROWS), F32),
        vm((2, 6 * TT, 256), F32),
        vm((ROWS, 256), F32),
        vm((ROWS, 256), BF16),
        vm((FF_DEV, HEAD), BF16),
        vm((FF_DEV, HEAD), BF16),
        pltpu.SemaphoreType.DMA((5,)),
        dma((2,)), dma((2, 16)), dma((6,)), dma((6, 16)), dma, dma((16,)),
        dma((2,)), dma((8,)), dma, dma((4,)), dma, dma((8,)), dma, dma((8,)),
        dma((2,)), dma((8,)), dma, dma((4,)), dma, dma((8,)),
        dma((5,)), dma((5,)), dma((2,)), dma((2,)), dma((2, 2)), dma((2, 2)),
    ]
    return pl.pallas_call(
        kernel,
        out_shape=jax.ShapeDtypeStruct((ROWS, 256), BF16),
        in_specs=[pl.BlockSpec(memory_space=pl.ANY if i in (0, 6, 8, 9, 10) else pltpu.VMEM) for i in range(15)],
        out_specs=pl.BlockSpec(memory_space=pltpu.VMEM),
        scratch_shapes=scratch,
        compiler_params=pltpu.CompilerParams(collective_id=0, has_side_effects=True, vmem_limit_bytes=60 * 1024 * 1024),
        name="layer",
    )(
        residual_in, queries, keys, values, query_gain.reshape(1, HEAD), key_norm_gain.reshape(1, HEAD), out_weight,
        mlp_gain.reshape(1, D), gate_weight.T, up_weight.T, down_weight, *tables,
    )


def solution(mesh):
    in_specs = (
        P("sp", "tp"), P("sp", "tp"), P("sp", None), P("sp", None), P(), P(), P("tp", None), P(),
        P("sp", "tp"), P("sp", "tp"), P("tp", "sp"),
    )
    return jax.shard_map(on_device, mesh=mesh, in_specs=in_specs, out_specs=P("sp", "tp"), check_vma=False)
```

```python
import functools
import math

import jax
import jax.numpy as jnp
import numpy as np
from jax import lax
from jax.experimental import pallas as pl
from jax.experimental.pallas import tpu as pltpu
from jax.sharding import PartitionSpec as P

D = 2048
HEAD = 128
GRID = 64
ROWS = 768
FF_DEV = 704
EPS = 1e-06
TT = ROWS // 8
HALF = ROWS // 2

LOG2E = 1.4426950408889634
SCORE = HEAD ** (-0.5) * LOG2E
MESH = pl.DeviceIdType.MESH
F32 = jnp.float32
BF16 = jnp.bfloat16

ORDER = [(0, 0), (0, 3), (1, 0), (0, 1), (3, 0), (0, 2), (1, 1), (2, 0), (1, 3), (3, 1), (3, 3), (1, 2), (2, 3), (2, 1), (3, 2), (2, 2)]
SCHEDULE = {
    "own": (("o", "gd", 0, 3),),
    "a1": (("o", "gd", 1, 0), ("ka", 0, 3), ("ka", 1, 0), ("ka", 3, 0), ("ka", 0, 1), ("o", "ga", 3, 0), ("kb", 0, 3), ("r", 0, 3), ("kb", 1, 0), ("r", 1, 0), ("kb", 0, 1), ("r", 0, 1), ("kb", 3, 0), ("r", 3, 0),),
    "a3": (("ka", 0, 2), ("gd", 0, 1), ("gd", 3, 0), ("ka", 1, 3),),
    "a4": (("ka", 3, 3), ("ga", 0, 1),),
    "a5": (("ka", 1, 1), ("kb", 0, 2), ("r", 0, 2), ("kb", 1, 1), ("r", 1, 1), ("ka", 2, 0), ("kb", 2, 0), ("r", 2, 0), ("kb", 1, 3), ("r", 1, 3),),
    "a7": (("ka", 3, 1), ("ka", 1, 2), ("kb", 3, 1), ("r", 3, 1), ("kb", 3, 3), ("r", 3, 3), ("o", "gd", 0, 1), ("o", "gc", 0, 1),),
    "a9": (("ka", 3, 2), ("gd", 3, 1), ("ka", 2, 3), ("gd", 3, 3), ("o", "gb", 3, 0), ("o", "gc", 1, 0),),
    "a10": (("kb", 1, 2), ("r", 1, 2),),
    "a11": (("kb", 2, 3), ("r", 2, 3), ("ga", 3, 1), ("ga", 1, 1), ("o", "gb", 1, 0),),
    "a12": (("kb", 2, 1), ("gc", 3, 0), ("o", "gc", 3, 0),),
    "a13": (("ka", 2, 1), ("r", 2, 1), ("gd", 0, 3), ("o", "gd", 3, 0), ("ka", 2, 2), ("kb", 3, 2), ("r", 3, 2), ("o", "ga", 0, 1), ("gc", 0, 3), ("o", "ga", 1, 0), ("gb", 1, 0),),
    "a15": (("kb", 2, 2), ("r", 2, 2), ("gb", 3, 0), ("ga", 2, 1), ("gd", 3, 2), ("o", "gc", 0, 3),),
    "p0": (("gc", 2, 0), ("gc", 0, 1), ("gd", 1, 0), ("gd", 0, 2),),
    "p1": (("ga", 3, 0), ("ga", 0, 3), ("gb", 1, 1), ("gc", 1, 3),),
    "p2": (("gc", 3, 3), ("gb", 3, 1), ("gb", 1, 3), ("gc", 1, 0), ("gb", 2, 0), ("gc", 0, 2), ("gb", 3, 3), ("gc", 1, 1), ("gd", 1, 1), ("gc", 3, 1), ("gd", 2, 0), ("gd", 1, 3),),
    "p4": (("gb", 1, 2), ("ga", 2, 0), ("ga", 0, 2), ("ga", 1, 3), ("o", "dd", 1, 0), ("o", "gb", 0, 1), ("gb", 3, 2), ("ga", 3, 3), ("gb", 2, 3), ("gc", 2, 3), ("gb", 2, 1), ("gc", 3, 2), ("o", "da", 3, 0), ("gc", 1, 2), ("gd", 2, 3), ("ga", 3, 2), ("gd", 1, 2), ("o", "dc", 3, 0), ("o", "gb", 0, 3), ("gb", 0, 3), ("gc", 2, 1), ("o", "ga", 0, 3), ("o", "dc", 1, 0), ("o", "db", 1, 0), ("o", "da", 1, 0), ("o", "db", 3, 0), ("o", "dd", 0, 1), ("o", "dd", 3, 0), ("o", "dc", 0, 3),),
    "p5": (("dd", 3, 0),),
    "p6": (("gd", 2, 1), ("ga", 1, 2), ("gb", 2, 2), ("gc", 2, 2), ("da", 0, 1), ("o", "dd", 0, 3), ("o", "db", 0, 3), ("dc", 0, 1), ("o", "db", 0, 1), ("ga", 2, 3), ("gd", 2, 2), ("ga", 2, 2),),
    "p7": (("gb", 0, 1), ("db", 3, 0), ("gb", 0, 2), ("ga", 1, 0), ("o", "da", 0, 1), ("o", "dc", 0, 1), ("o", "da", 0, 3),),
    "g0": (("dd", 2, 0), ("dd", 3, 1), ("dc", 0, 3), ("db", 1, 0), ("da", 0, 2), ("da", 3, 1),),
    "g1": (("dd", 1, 0), ("dc", 3, 1), ("dd", 0, 1), ("da", 0, 3),),
    "g2": (("db", 0, 1), ("db", 2, 0), ("dc", 1, 0), ("dd", 0, 3), ("dd", 3, 3), ("da", 1, 1),),
    "g3": (("dc", 0, 2), ("dc", 1, 1), ("da", 3, 0), ("db", 0, 3),),
    "g4": (("db", 3, 3), ("dc", 3, 0), ("da", 1, 0), ("db", 3, 1), ("dc", 3, 3), ("dd", 2, 1),),
    "p9": (("dc", 1, 3), ("dd", 2, 3), ("dd", 3, 2), ("da", 3, 2),),
    "i0": (("da", 1, 2), ("db", 1, 3),),
    "i1": (("da", 3, 3), ("db", 1, 1),),
    "i2": (("da", 1, 3), ("dd", 1, 3),),
    "i3": (("dc", 3, 2), ("dd", 1, 1),),
    "i4": (("db", 2, 3), ("da", 2, 1),),
    "p12": (("db", 2, 1), ("da", 2, 0), ("dc", 1, 2), ("dd", 0, 2), ("dc", 2, 0), ("db", 3, 2), ("db", 0, 2), ("dc", 2, 1), ("da", 2, 2), ("db", 1, 2), ("dc", 2, 3), ("dd", 2, 2), ("dc", 2, 2), ("dd", 1, 2), ("da", 2, 3), ("db", 2, 2),),
}
FAR_AT = 3
MIRRORED = ("kb", "gc", "gd", "da", "dc")


def rotary_tables():
    half = HEAD // 2
    freq = (10000.0 ** (-np.arange(0, half, 2, dtype=np.float32) / np.float32(half))).astype(np.float32)
    lanes = np.arange(HEAD)
    of_row = (lanes % 64) < 32
    sign = np.where(lanes < 64, -1.0, 1.0)
    f = freq[lanes % 32]
    out = []
    for count, mask in ((12288 // GRID, of_row), (GRID, ~of_row)):
        ang = (np.arange(count, dtype=np.float32)[:, None] * f[None, :]).astype(np.float32).astype(np.float64)
        out.append(np.where(mask, np.cos(ang), 0.0).astype(np.float32))
        out.append(np.where(mask, np.sin(ang) * sign, 0.0).astype(np.float32))
    return out


def kernel(
    res_h, q_ref, k_ref, v_ref, qg_ref, kg_ref, wo_h, mg_ref, g_h, u_h, dw_h,
    rc_ref, rs_ref, cc_ref, cs_ref,
    out_ref,
    kv, gu, dn, att, att_t, wo, res_t, mid_s, xn, pj, pr, hid, tb, rb, sb, pb, fb, qT, m_s, acc, scores, gu_s, base_s, res_ref, g_ref, u_ref, in_s,
    kv_ss, kv_rs, w_ss, w_rs, rel_ss, rel_rs, wo_ss, wo_rs, wd_ss, wd_rs, res_ss, res_rs, at_ss, at_rs,
    xs_ss, xs_rs, xd_ss, xd_rs, pj_ss, pj_rs, td_ss, td_rs, p_ss, p_rs, f_ss, f_rs,
):
    sp = lax.axis_index("sp")
    tp = lax.axis_index("tp")
    z, y = sp // 4, sp % 4
    x, core = tp // 2, tp % 2

    def bid(a, b):
        return ((z + a) % 4) * 4 + (y + b) % 4

    def near(dz, dy):
        return {"sp": bid(dz, dy), "tp": tp}

    def xdev(dx):
        return {"sp": sp, "tp": ((x + dx) % 4) * 2 + core}

    partner_tp = x * 2 + 1 - core
    partner = {"sp": sp, "tp": partner_tp}

    def copy(src, dst, ss, rs, dev):
        return pltpu.make_async_remote_copy(src_ref=src, dst_ref=dst, send_sem=ss, recv_sem=rs, device_id=dev, device_id_type=MESH)

    barrier = pltpu.get_barrier_semaphore()
    peers = [near(0, 1), near(0, 3), near(1, 0), near(3, 0)]
    peers += [{"sp": sp, "tp": (tp + d) % 8} for d in range(1, 8)]
    for dev in peers:
        pl.semaphore_signal(barrier, inc=1, device_id=dev, device_id_type=MESH)

    loads = [
        pltpu.make_async_copy(res_h, res_ref, in_s.at[0]),
        pltpu.make_async_copy(wo_h, wo.at[tp], in_s.at[1]),
        pltpu.make_async_copy(g_h, g_ref, in_s.at[2]),
        pltpu.make_async_copy(u_h, u_ref, in_s.at[3]),
        pltpu.make_async_copy(dw_h, dn.at[sp, 0:FF_DEV], in_s.at[4]),
    ]
    for load in loads:
        load.start()

    def rotated(ref, lane0, gain, g):
        t = ref[g * 64 : (g + 1) * 64, pl.ds(lane0, HEAD)].astype(F32)
        t = t * lax.rsqrt(jnp.mean(t * t, axis=1, keepdims=True) + EPS) * gain
        grid_row = sp * (ROWS // GRID) + g
        cos = rc_ref[pl.ds(grid_row, 1), :] + cc_ref[...]
        sin = rs_ref[pl.ds(grid_row, 1), :] + cs_ref[...]
        return t * cos + pltpu.roll(t, 64, 1) * sin

    lane0 = pl.multiple_of((tp // 4) * HEAD, HEAD)
    kgain = kg_ref[...]
    qgain = qg_ref[...]
    def own_keys():
        for g in range(ROWS // GRID):
            kv[0, sp, g // 2, pl.ds((g % 2) * 64, 64), :] = rotated(k_ref, lane0, kgain, g).astype(BF16)

    def own_values():
        for i in range(6):
            vi = v_ref[i * 128 : (i + 1) * 128, pl.ds(lane0, HEAD)].astype(F32)
            kv[1, sp, i] = vi.T.astype(BF16)

    pl.when(core == 0)(own_keys)
    pl.when(core == 1)(own_values)

    with jax.named_scope("barrier"):
        pl.semaphore_wait(barrier, len(peers))

    pieces = {
        "ka": (lambda i: kv.at[core, i, 0:3], kv_ss.at[0], kv_rs.at[0]),
        "kb": (lambda i: kv.at[core, i, 3:6], kv_ss.at[1], kv_rs.at[1]),
    }
    for n, name in enumerate(("da", "db", "dc", "dd")):
        pieces[name] = (lambda i, n=n: dn.at[i, n * 176 : (n + 1) * 176], w_ss.at[4 + n], w_rs.at[4 + n])
    for n, name in enumerate(("ga", "gb", "gc", "gd")):
        pieces[name] = (lambda i, n=n: gu.at[i, n * 32 : (n + 1) * 32], w_ss.at[n], w_rs.at[n])

    def send(name, a, b, du, dw):
        piece, ss, rs = pieces[name]
        dz, dy = (dw, du) if name[1] in "ac" else (du, dw)
        ref = piece(bid(a, b))
        copy(ref, ref, ss, rs.at[((a - dz) % 4) * 4 + (b - dy) % 4], near(dz, dy)).start()

    def take(name, a, b):
        piece, ss, rs = pieces[name]
        ref = piece(bid(a, b))
        copy(ref, ref, ss, rs.at[a * 4 + b], near(0, 1)).wait_recv()
        u, w = (b, a) if name[1] in "ac" else (a, b)
        if w == 0 and u == 3 and name not in MIRRORED:
            send(name, a, b, 1, 0)
        if w == 0 and u == 1 and name in MIRRORED:
            send(name, a, b, 3, 0)
        if w == 0 or (w == 3 and u % 2 == 0):
            send(name, a, b, 0, 1)
        if w == 0 or (w == 1 and u % 2 == 1):
            send(name, a, b, 0, 3)

    def drain(name):
        piece, ss, rs = pieces[name]
        ref = piece(pl.ds(0, 15))
        copy(ref, ref, ss, rs.at[0], near(0, 1)).wait_send()

    def run(gap):
        with jax.named_scope(f"run_{gap}"):
            for item in SCHEDULE.get(gap, ()):
                if item[0] == "o":
                    send(item[1], 0, 0, item[2], item[3])
                elif item[0] == "r":
                    ref = kv.at[core, bid(item[1], item[2])]
                    copy(ref, ref, rel_ss, rel_rs.at[item[1] * 4 + item[2]], partner).start()
                else:
                    take(*item)

    def kv_relayed(a, b):
        ref = kv.at[1 - core, bid(a, b)]
        copy(ref, ref, rel_ss, rel_rs.at[a * 4 + b], partner).wait_recv()

    for name in ("ka", "kb"):
        for du, dw in ((1, 0), (3, 0), (0, 1), (0, 3)):
            send(name, 0, 0, du, dw)

    pl.when(core == 1)(own_keys)
    pl.when(core == 0)(own_values)

    def tokens(i):
        return pl.ds(pl.multiple_of(i * TT, TT), TT)

    def exchange(src, dst, ss, rs):
        for d in (1, 2, 7, 6, 3, 5, 4):
            to = (tp + d) % 8
            copy(src(to), dst(tp), ss, rs.at[8 - d], {"sp": sp, "tp": to}).start()

    def exchanged(dst, ss, rs):
        for d in range(1, 8):
            frm = (tp + d) % 8
            copy(dst(frm), dst(frm), ss, rs.at[d], {"sp": sp, "tp": frm}).wait_recv()

    def exchange_drain(dst, ss, rs):
        ref = dst(pl.ds(0, 7))
        copy(ref, ref, ss, rs.at[0], partner).wait_send()

    for load in loads:
        load.wait()
    exchange(lambda i: res_ref.at[tokens(i)], lambda i: res_t.at[i], res_ss, res_rs)

    for g in range(ROWS // GRID):
        qT[:, g * 64 : (g + 1) * 64] = rotated(q_ref, 0, qgain, g).T.astype(BF16)
    m_s[...] = jnp.full_like(m_s, -1e30)
    acc[...] = jnp.zeros_like(acc)

    for n in range(5):
        cols = slice(n * 128, (n + 1) * 128)
        gu[sp, :, n * 256 : n * 256 + 128] = g_ref[cols, :].T
        gu[sp, :, n * 256 + 128 : (n + 1) * 256] = u_ref[cols, :].T
    gu[sp, :, 1280:1408] = jnp.concatenate([g_ref[640:704, :], u_ref[640:704, :]], axis=0).T
    for i in range(16):
        dn[i, 704:768, :] = jnp.zeros((64, 128), BF16)

    def xgather(block, pieces, ss, rs, dss, drs):
        def own(dx):
            return ((x + dx) % 4) * 2 + core

        def send(dx, p, to):
            ref = block(own(dx), pieces[p])
            copy(ref, ref, ss.at[p], rs.at[((dx - to) % 4) * 2 + p], xdev(to)).start()

        def wait(dx, p):
            ref = block(own(dx), pieces[p])
            copy(ref, ref, ss.at[p], rs.at[(dx % 4) * 2 + p], xdev(1)).wait_recv()

        whole = (0, pieces[1][1])

        def relay(dx):
            ref = block(own(dx), whole)
            copy(ref, ref, dss, drs.at[dx % 4], partner).start()

        def start():
            send(0, 0, 1)
            send(0, 1, 3)
            send(0, 1, 1)
            send(0, 0, 3)
            relay(0)

        def forward():
            wait(3, 0)
            send(3, 0, 1)
            wait(1, 1)
            send(1, 1, 3)

        def finish():
            wait(3, 1)
            relay(3)
            wait(1, 0)
            relay(1)

        def finish_far():
            wait(2, 0)
            wait(2, 1)
            relay(2)

        def relayed(which=(0, 3, 1, 2)):
            for dx in which:
                ref = block(((x + dx) % 4) * 2 + 1 - core, whole)
                copy(ref, ref, dss, drs.at[dx], partner).wait_recv()

        def drain():
            for p in range(2):
                ref = block(pl.ds(0, 3), pieces[p])
                copy(ref, ref, ss.at[p], rs.at[0], xdev(1)).wait_send()
            ref = block(pl.ds(0, 4), whole)
            copy(ref, ref, dss, drs.at[0], partner).wait_send()

        return start, forward, finish, finish_far, relayed, drain

    def rows_of(ref):
        return lambda i, r: ref.at[i, r[0] : r[1]]

    wo_start, wo_forward, wo_finish, wo_far, wo_relayed, wo_drain = xgather(
        rows_of(wo), ((0, 64), (64, HEAD)), wo_ss, wo_rs, wd_ss, wd_rs
    )
    xn_start, xn_forward, xn_finish, xn_far, xn_relayed, xn_drain = xgather(
        rows_of(xn), ((0, TT // 2), (TT // 2, TT)), xs_ss, xs_rs, xd_ss, xd_rs
    )
    wo_start()

    def product(blk):
        return jnp.dot(kv[0, blk].reshape(ROWS, HEAD), qT[...], preferred_element_type=F32)

    def absorb(s, blk):
        old = m_s[...]
        new = jnp.maximum(old, jnp.max(s, axis=0, keepdims=True))
        factor = jnp.exp2((old - new) * SCORE)
        m_s[...] = new
        p = jnp.exp2((s - new) * SCORE).astype(BF16)
        v = kv[1, blk]
        vt = jnp.concatenate([v[i] for i in range(6)], axis=1)
        vt = jnp.concatenate([vt, jnp.ones((16, ROWS), BF16)], axis=0)
        acc[...] = acc[...] * factor + jnp.dot(vt, p, preferred_element_type=F32)

    def place(s):
        a, b = jnp.int32(0), jnp.int32(0)
        for i, (ai, bi) in enumerate(ORDER):
            a = jnp.where(s == i, ai, a)
            b = jnp.where(s == i, bi, b)
        return a, b

    run("own")
    with jax.named_scope("att_own"):
        absorb(product(sp), sp)
    run("a1")
    with jax.named_scope("relay_wait"):
        kv_relayed(*ORDER[1])
    with jax.named_scope("first"):
        scores[0] = product(bid(*ORDER[1]))

    def att_loop(i, c):
        for h in range(2):
            s = 2 * i + 1 + h
            for k in range(2 + h, 16, 2):
                pl.when(s == k - 1)(functools.partial(run, f"a{k}"))
            for k, fn in ((3, wo_forward), (9, wo_finish), (13, wo_far)):
                if k % 2 == 1 - h:
                    pl.when(s == k)(fn)
            now, later = place(s), place(s + 1)
            with jax.named_scope("relay_wait"):
                kv_relayed(*later)
            with jax.named_scope("attend"):
                scores[1 - h] = product(bid(*later))
                absorb(scores[h], bid(*now))
        return c

    lax.fori_loop(0, 7, att_loop, 0)
    absorb(scores[0], bid(*ORDER[15]))
    run("p0")
    with jax.named_scope("att_out"):
        attn = (acc[0:HEAD, :] / acc[HEAD : HEAD + 1, :]).T.astype(BF16)
        att[...] = attn

    exchange(lambda i: att.at[tokens(i)], lambda i: att_t.at[i], at_ss, at_rs)
    att_t[tp] = att[tokens(tp)]
    res_t[tp] = res_ref[tokens(tp), :]
    run("p1")
    with jax.named_scope("wo_wait"):
        wo_relayed()
        exchanged(lambda i: res_t.at[i], res_ss, res_rs)
    run("p2")
    with jax.named_scope("att_wait"):
        exchanged(lambda i: att_t.at[i], at_ss, at_rs)

    def project():
        left = jnp.concatenate([att_t[i] for i in range(8)], axis=1)
        squares = jnp.zeros((TT, 1), F32)
        for n in range(4):
            cols = slice(n * 512, (n + 1) * 512)
            p = jnp.dot(left, wo[:, :, cols].reshape(8 * HEAD, 512), preferred_element_type=F32)
            for i in range(2):
                part = p[:, i * 256 : (i + 1) * 256]
                pj[2 * n + i] = part.astype(BF16)
                mid = res_t[2 * n + i].astype(F32) + part
                mid_s[:, n * 512 + i * 256 : n * 512 + (i + 1) * 256] = mid
                squares = squares + jnp.sum(mid * mid, axis=1, keepdims=True)
        scale = lax.rsqrt(squares / D + EPS)
        xn[tp] = (mid_s[...] * scale * mg_ref[...]).astype(BF16)

    with jax.named_scope("project"):
        project()
    xn_start()

    def gate_up(far_by, name):
        chips = [(x + dx) % 4 for dx in far_by]

        def keep(value, lanes):
            for i, c in enumerate(chips):
                rows = pl.ds(pl.multiple_of(c * 2 * TT, 2 * TT), 2 * TT)
                hid[rows, lanes] = value[i * 2 * TT : (i + 1) * 2 * TT].astype(BF16)

        count = len(chips) * 2 * TT

        def silu(n):
            o = gu_s[n % 2, 0:count, :]
            if n < 5:
                gate, up = o[:, 0:128], o[:, 128:256]
                keep(gate / (1.0 + jnp.exp(-gate)) * up, slice(n * 128, (n + 1) * 128))
            else:
                o = o[:, 0:128]
                tail = o / (1.0 + jnp.exp(-o)) * pltpu.roll(o, 64, 1)
                lane = lax.broadcasted_iota(jnp.int32, tail.shape, 1)
                keep(jnp.where(lane < 64, tail, 0.0), slice(640, 768))

        for n in range(6):
            width = 256 if n < 5 else 128
            w = gu[:, :, n * 256 : n * 256 + width].reshape(D, width)
            for i, c in enumerate(chips):
                left = xn[pl.ds(2 * c, 2)].reshape(2 * TT, D)
                gu_s[n % 2, i * 2 * TT : (i + 1) * 2 * TT, 0:width] = jnp.dot(left, w, preferred_element_type=F32)
            if n > 0:
                silu(n - 1)
            if n < 5:
                run(f"{name}{n}")
                if name == "g" and n == FAR_AT:
                    run("gf")
                    with jax.named_scope("xn_far"):
                        xn_far()
        silu(5)

    def down(dx, rows=slice(0, ROWS)):
        j = ((x + dx) % 4) * 4
        w = jnp.concatenate([dn[j + i] for i in range(4)], axis=1)
        o = jnp.dot(hid[rows, :], w, preferred_element_type=F32)
        for c in range(2):
            tb[dx, c, rows] = o[:, c * 256 : (c + 1) * 256].astype(BF16)

    def to_partner(dx):
        return copy(tb.at[dx, 1 - core], rb.at[dx], td_ss.at[dx], td_rs.at[dx], partner)

    def half_to_partner(h):
        rows = pl.ds(h * HALF, HALF)
        return copy(tb.at[2, 1 - core, rows], rb.at[2, rows], td_ss.at[2 + 2 * h], td_rs.at[2 + 2 * h], partner)

    def far(i):
        to = xdev((1, 3)[i])
        return copy(sb.at[0, pl.ds(i * HALF, HALF)], pb.at[i], p_ss.at[i], p_rs.at[i], to)

    def close(i, h):
        to = xdev((1, 3)[i])
        rows = pl.ds(h * HALF, HALF)
        return copy(sb.at[1 + i, rows], fb.at[i, rows], f_ss.at[i, h], f_rs.at[i, h], to)

    def both(dx, h):
        rows = slice(h * HALF, (h + 1) * HALF)
        return tb[dx, core, rows].astype(F32) + rb[dx, rows].astype(F32)

    def reduce_far(i):
        half_to_partner(i).wait_recv()
        sb[0, i * HALF : (i + 1) * HALF] = both(2, i).astype(BF16)
        far(i).start()

    def reduce_free(i):
        dx, h = (1, 3)[i], 1 - i
        to_partner(dx).wait_recv()
        sb[1 + i, h * HALF : (h + 1) * HALF] = both(dx, h).astype(BF16)
        close(i, h).start()

    def reduce_near(i):
        dx, h = (1, 3)[i], i
        s = both(dx, h)
        far(i).wait_recv()
        sb[1 + i, h * HALF : (h + 1) * HALF] = (s + pb[i].astype(F32)).astype(BF16)
        close(i, h).start()

    def begin(h):
        rows = slice(h * HALF, (h + 1) * HALF)
        i = 1 - h
        close(i, h).wait_recv()
        mid = res_ref[rows, :].astype(F32) + pr[h * 4 : h * 4 + 4].reshape(HALF, 256).astype(F32)
        base_s[rows, :] = mid + 0.5 * (both(0, h) + fb[i, rows].astype(F32))

    def final(h):
        rows = slice(h * HALF, (h + 1) * HALF)
        close(h, h).wait_recv()
        out_ref[rows, :] = (base_s[rows, :] + 0.5 * fb[h, rows].astype(F32)).astype(BF16)

    run("p4")
    with jax.named_scope("xn_forward"):
        xn_forward()
    with jax.named_scope("exchangelambdaipja"):
        exchange(lambda i: pj.at[i], lambda i: pr.at[i], pj_ss, pj_rs)
    with jax.named_scope("prtppjtp"):
        pr[tp] = pj[tp]
    run("p5")
    with jax.named_scope("xn_relayed_own"):
        xn_relayed((0,))
    run("p6")
    with jax.named_scope("xn_finish"):
        xn_finish()
    run("p7")
    with jax.named_scope("xn_relayed"):
        xn_relayed((3, 1))
    run("p8")
    with jax.named_scope("gate_up"):
        gate_up((0, 3, 1), "g")
    run("p9")
    with jax.named_scope("xn_relayed_far"):
        xn_relayed((2,))
    with jax.named_scope("gate_up_far"):
        gate_up((2,), "i")
    run("p12")
    with jax.named_scope("down2"):
        down(2, slice(0, HALF))
        half_to_partner(0).start()
        down(2, slice(HALF, ROWS))
        half_to_partner(1).start()
    with jax.named_scope("down1"):
        down(1)
        to_partner(1).start()
    with jax.named_scope("reduce_far"):
        reduce_far(0)
        reduce_far(1)
    with jax.named_scope("down3"):
        down(3)
        to_partner(3).start()
    with jax.named_scope("reduce_free0"):
        reduce_free(0)
    with jax.named_scope("reduce_free1"):
        reduce_free(1)
    with jax.named_scope("down0"):
        down(0)
        to_partner(0).start()
    with jax.named_scope("reduce_near0"):
        reduce_near(0)
    with jax.named_scope("reduce_near1"):
        reduce_near(1)
    with jax.named_scope("to_partner0wait_re"):
        to_partner(0).wait_recv()
    with jax.named_scope("exchangedlambdaipr"):
        exchanged(lambda i: pr.at[i], pj_ss, pj_rs)
    with jax.named_scope("begin"):
        begin(0)
        begin(1)
    with jax.named_scope("final0"):
        final(0)
    with jax.named_scope("final1"):
        final(1)

    with jax.named_scope("drain"):
        for name in pieces:
            drain(name)
    ref = kv.at[0, 0:15]
    copy(ref, ref, rel_ss, rel_rs.at[0], partner).wait_send()
    exchange_drain(lambda i: res_t.at[i], res_ss, res_rs)
    exchange_drain(lambda i: att_t.at[i], at_ss, at_rs)
    exchange_drain(lambda i: pr.at[i], pj_ss, pj_rs)
    wo_drain()
    xn_drain()
    for dx in (0, 1, 3):
        to_partner(dx).wait_send()
    for i in range(2):
        half_to_partner(i).wait_send()
        far(i).wait_send()
        close(i, 0).wait_send()
        close(i, 1).wait_send()


def on_device(residual_in, queries, keys, values, query_gain, key_norm_gain, out_weight, mlp_gain, gate_weight, up_weight, down_weight):
    tables = [jnp.asarray(t) for t in rotary_tables()]
    dma = pltpu.SemaphoreType.DMA
    vm = pltpu.VMEM
    scratch = [
        vm((2, 16, 6, 128, 128), BF16),
        vm((16, 128, 2 * FF_DEV), BF16),
        vm((16, 768, 128), BF16),
        vm((ROWS, HEAD), BF16),
        vm((8, TT, HEAD), BF16),
        vm((8, HEAD, D), BF16),
        vm((8, TT, 256), BF16),
        vm((TT, D), F32),
        vm((8, TT, D), BF16),
        vm((8, TT, 256), BF16),
        vm((8, TT, 256), BF16),
        vm((ROWS, 768), BF16),
        vm((4, 2, ROWS, 256), BF16),
        vm((4, ROWS, 256), BF16),
        vm((3, ROWS, 256), BF16),
        vm((2, HALF, 256), BF16),
        vm((2, ROWS, 256), BF16),
        vm((HEAD, ROWS), BF16),
        vm((1, ROWS), F32),
        vm((HEAD + 16, ROWS), F32),
        vm((2, ROWS, ROWS), F32),
        vm((2, 6 * TT, 256), F32),
        vm((ROWS, 256), F32),
        vm((ROWS, 256), BF16),
        vm((FF_DEV, HEAD), BF16),
        vm((FF_DEV, HEAD), BF16),
        pltpu.SemaphoreType.DMA((5,)),
        dma((2,)), dma((2, 16)), dma((8,)), dma((8, 16)), dma, dma((16,)),
        dma((2,)), dma((8,)), dma, dma((4,)), dma, dma((8,)), dma, dma((8,)),
        dma((2,)), dma((8,)), dma, dma((4,)), dma, dma((8,)),
        dma((5,)), dma((5,)), dma((2,)), dma((2,)), dma((2, 2)), dma((2, 2)),
    ]
    return pl.pallas_call(
        kernel,
        out_shape=jax.ShapeDtypeStruct((ROWS, 256), BF16),
        in_specs=[pl.BlockSpec(memory_space=pl.ANY if i in (0, 6, 8, 9, 10) else pltpu.VMEM) for i in range(15)],
        out_specs=pl.BlockSpec(memory_space=pltpu.VMEM),
        scratch_shapes=scratch,
        compiler_params=pltpu.CompilerParams(collective_id=0, has_side_effects=True, vmem_limit_bytes=60 * 1024 * 1024),
        name="layer",
    )(
        residual_in, queries, keys, values, query_gain.reshape(1, HEAD), key_norm_gain.reshape(1, HEAD), out_weight,
        mlp_gain.reshape(1, D), gate_weight.T, up_weight.T, down_weight, *tables,
    )


def solution(mesh):
    in_specs = (
        P("sp", "tp"), P("sp", "tp"), P("sp", None), P("sp", None), P(), P(), P("tp", None), P(),
        P("sp", "tp"), P("sp", "tp"), P("tp", "sp"),
    )
    return jax.shard_map(on_device, mesh=mesh, in_specs=in_specs, out_specs=P("sp", "tp"), check_vma=False)
```
